128 devices in a mesh: sp: 32 (over z, y, core), tp: 4 (over x).
Axes of the slice: x: 4, y: 4, z: 4, core: 2. Of those that a mesh axis runs over, the one named last changes fastest.
Arguments:
- tokens: bfloat16 [4096, 6, 2048], P(('sp', 'tp')), may hold values from -6 to 6
- norm_gain: float32 [2048], replicated, may hold values from 0.1 to 1.9
- w_query: bfloat16 [3, 2048, 1024], P(None, 'sp', 'tp'), may hold values from -0.125 to 0.125
- w_key: bfloat16 [3, 2048, 1024], P(None, 'sp', 'tp'), may hold values from -0.125 to 0.125
- w_value: bfloat16 [3, 2048, 1024], P(None, 'sp', 'tp'), may hold values from -0.125 to 0.125
- w_out: bfloat16 [1024, 2048], P('tp', 'sp'), may hold values from -0.1875 to 0.1875
Outputs:
- mixed: bfloat16 [4096, 6, 2048], P(('sp', 'tp'))
- log_weight: float32 [4096, 6, 8], P('sp', None, 'tp')
The draws below stay inside these ranges and needn't reach their ends.
All inputs are finite; a program needn't handle non-finite values.
Results may differ from the reference program's by a relative error of at most 0.015.
Values may be sent and summed in bfloat16 or wider, within the bound.
No kernel may reach another device: no remote copies, remote signals or barrier semaphores. Data moves between devices by JAX's collectives and lax.ppermute only.
A program may use at most 128 MiB of HBM per device.

```python
import jax
import jax.numpy as jnp
from jax import lax

WIDTH = 2048
GROUPS = 3
HEADS = 8
HEAD_WIDTH = 128
STEPS = 24
DILATION_MIDDLE = 4
DILATION_WIDE = 16
BATCH = 6
LENGTH = 4096


def shard_levels(own_key, dims, pieces, least, high):
    def one(dim, blocks):
        draws = jax.random.uniform(jax.random.fold_in(jax.random.fold_in(own_key, 6), dim), (blocks,), jnp.float32, least / len(pieces), high / len(pieces))
        return jnp.repeat(jnp.exp(draws), dims[dim] // blocks).reshape((-1,) + (1,) * (len(dims) - dim - 1))

    factor_of = one(*pieces[0])
    for cut in pieces[1:]:
        factor_of = factor_of * one(*cut)
    return factor_of


def normal_values(rng, dims, spread, limit, cuts=(), kind=jnp.bfloat16):
    array = jax.random.normal(rng, dims, jnp.float32) * spread
    if len(cuts) > 0:
        array = shard_levels(rng, dims, cuts, -0.22, 0.18) * array
    return jnp.clip(array, min=-limit, max=limit).astype(kind)


def setup_inputs(seed: int = 0) -> dict:
    splits = jax.random.split(jax.random.key(seed), 7)
    tokens = normal_values(splits[0], (LENGTH, BATCH, WIDTH), 1.0, 6.0, ((0, 128),))
    norm_gain = jnp.clip(1.0 + 0.18 * jax.random.normal(splits[1], (WIDTH,), jnp.float32), 0.1, 1.9)
    w_query = normal_values(splits[2], (GROUPS, WIDTH, HEADS * HEAD_WIDTH), WIDTH ** -0.5, 0.125, ((1, 32), (2, 4)))
    w_key = normal_values(splits[3], (GROUPS, WIDTH, HEADS * HEAD_WIDTH), WIDTH ** -0.5, 0.125, ((1, 32), (2, 4)))
    w_value = normal_values(splits[4], (GROUPS, WIDTH, HEADS * HEAD_WIDTH), WIDTH ** -0.5, 0.125, ((1, 32), (2, 4)))
    w_out = normal_values(splits[5], (HEADS * HEAD_WIDTH, WIDTH), (HEADS * HEAD_WIDTH) ** -0.5, 0.1875, ((0, 4), (1, 32)))
    return dict(tokens=tokens, norm_gain=norm_gain, w_query=w_query, w_key=w_key, w_value=w_value, w_out=w_out)


epsilon = 1e-06

def rms_normed(values, gain):
    widened = values.astype(jnp.float32)
    scaled = widened * lax.rsqrt(lax.optimization_barrier(jnp.mean(widened * widened, axis=-1, keepdims=True)) + epsilon)
    return (scaled * gain.astype(jnp.float32)).astype(jnp.bfloat16)

def reference(tokens, norm_gain, w_query, w_key, w_value, w_out):
    seq_count, batch_count, width_count = tokens.shape
    normed = rms_normed(tokens, norm_gain)
    flat_rows = normed.reshape(seq_count * batch_count, width_count)
    positions = jnp.arange(seq_count, dtype=jnp.int32)
    scale = 1.0 / HEAD_WIDTH ** 0.5
    group_logs = []
    group_outs = []
    for group_index, dilation in enumerate((1, DILATION_MIDDLE, DILATION_WIDE)):

        def project(weight):
            product = jnp.dot(flat_rows, weight[group_index], preferred_element_type=jnp.float32)
            return product.astype(jnp.bfloat16).reshape(seq_count, batch_count, HEADS, HEAD_WIDTH).astype(jnp.float32)
        queries = project(w_query)
        keys = project(w_key)
        values = project(w_value)
        score_list = []
        for lag_index in range(STEPS + 1):
            offset = lag_index * dilation
            moved = jnp.pad(keys, ((offset, 0), (0, 0), (0, 0), (0, 0)))[:seq_count]
            score = jnp.einsum('sbhe,sbhe->sbh', queries, moved, precision=lax.Precision.HIGHEST) * scale
            score_list.append(jnp.where((positions >= offset)[:, None, None], score, jnp.float32(-1e+30)))
        scores = jnp.stack(score_list)
        peak = lax.optimization_barrier(jnp.max(scores, axis=0))
        lifted = jnp.exp(scores - peak[None])
        totals = lax.optimization_barrier(jnp.sum(lifted, axis=0))
        group_logs.append(peak + jnp.log(totals))
        probs = (lifted / totals[None]).astype(jnp.bfloat16).astype(jnp.float32)
        accumulated = jnp.zeros((seq_count, batch_count, HEADS, HEAD_WIDTH), jnp.float32)
        for lag_index in range(STEPS + 1):
            offset = lag_index * dilation
            moved = jnp.pad(values, ((offset, 0), (0, 0), (0, 0), (0, 0)))[:seq_count]
            accumulated = accumulated + probs[lag_index][..., None] * moved
        group_outs.append(accumulated.astype(jnp.bfloat16))
    stacked_logs = jnp.stack(group_logs)
    top_log = lax.optimization_barrier(jnp.max(stacked_logs, axis=0))
    log_weight = top_log + jnp.log(lax.optimization_barrier(jnp.sum(jnp.exp(stacked_logs - top_log[None]), axis=0)))
    shares = jax.nn.softmax(stacked_logs, axis=0)
    outputs = jnp.stack(group_outs).astype(jnp.float32)
    combined = lax.optimization_barrier(jnp.sum(shares[..., None] * outputs, axis=0)).astype(jnp.bfloat16)
    combined = combined.reshape(seq_count * batch_count, HEADS * HEAD_WIDTH)
    mixed = jnp.dot(combined, w_out, preferred_element_type=jnp.float32).astype(jnp.bfloat16)
    return (mixed.reshape(seq_count, batch_count, width_count), log_weight)
```

```python
import math

import jax
import jax.numpy as jnp
from jax import lax
from jax.experimental import pallas as pl
from jax.experimental.pallas import tpu as pltpu
from jax.sharding import PartitionSpec as P

GROUPS = 3
HEADS = 8
STEPS = 24
DILATIONS = (1, 4, 16)
HALOS = (32, 96, 384)
RING = 4
BATCHES = 3
PIECE = 32
SPAN = 256
HEAD_WIDTH = 128
COLS = 256
ROWS = 64
WIDTH = 2048
BLOCK = 128

epsilon = 1e-06


def chip(z, y, core):
    return (z % RING) * 8 + (y % RING) * 2 + core


def chips():
    return [(z, y, core) for z in range(RING) for y in range(RING) for core in range(2)]


def first_leg(shift):
    return [(chip(z, y, k), chip(z + shift * k, y + shift * (1 - k), k)) for z, y, k in chips()]


def second_leg(shift):
    return [(chip(z, y, k), chip(z + shift * (1 - k), y + shift * k, k)) for z, y, k in chips()]


SWAP = [(i, i ^ 1) for i in range(32)]


def swapped(a):
    return lax.ppermute(a, "sp", SWAP)


def turned(a, shift):
    return lax.ppermute(a, "tp", [(i, (i + shift) % RING) for i in range(RING)])


def from_behind(a, blocks):
    return lax.ppermute(a, "sp", [(i, i + 2 * blocks) for i in range(32 - 2 * blocks)])


def spread(own):
    near = [own] + [lax.ppermute(own, "sp", first_leg(d)) for d in (1, 3, 2)]
    line = jnp.stack((near[0], near[1], near[3], near[2]))
    far = [lax.ppermute(line, "sp", second_leg(d)) for d in (1, 3, 2)]
    return [line, far[0], far[2], far[1]]


def place_of(core, first, second):
    s = lax.axis_index("sp")
    z, y = s // 8, (s // 2) % RING
    up = jnp.where(core == 0, second, first)
    along = jnp.where(core == 0, first, second)
    return ((z + RING - up) % RING) * 8 + ((y + RING - along) % RING) * 2 + core


ANY = pl.BlockSpec(memory_space=pl.ANY)
VMEM = pl.BlockSpec(memory_space=pltpu.VMEM)
PARAMS = pltpu.CompilerParams(vmem_limit_bytes=56 * 1024 * 1024)


def norm_body(tokens, gain, keep, send):
    core = lax.axis_index("sp") % 2
    widened_gain = gain[...]
    for b in range(2 * BATCHES):
        v = tokens[:, b, :].astype(jnp.float32)
        v = v * lax.rsqrt(jnp.mean(v * v, axis=-1, keepdims=True) + epsilon)
        n = (v * widened_gain).astype(jnp.bfloat16)

        @pl.when(core == b // BATCHES)
        def _():
            keep[b % BATCHES] = n

        @pl.when(core != b // BATCHES)
        def _():
            send[b % BATCHES] = n


def norm_rows(tokens, gain):
    shape = jax.ShapeDtypeStruct((BATCHES, PIECE, WIDTH), jnp.bfloat16)
    return pl.pallas_call(
        norm_body, out_shape=(shape, shape), in_specs=[VMEM, VMEM], out_specs=(VMEM, VMEM),
        compiler_params=PARAMS, name="norm_rows",
    )(tokens, gain.reshape(1, WIDTH))


def fetch(pieces, lines, x_all, w_all, x_sems, w_sems, matrices):
    s, t = lax.axis_index("sp"), lax.axis_index("tp")
    core = s % 2
    copies = []
    for n, piece in enumerate(pieces):
        whose = core if n < RING else 1 - core
        at = whose * (RING * PIECE) + ((t + RING - n % RING) % RING) * PIECE
        at = pl.multiple_of(at, PIECE)
        copies.append(pltpu.make_async_copy(piece, x_all.at[:, pl.ds(at, PIECE), :], x_sems.at[n]))
    for n, line in enumerate(lines):
        whose = core if n < RING else 1 - core
        for j in range(RING):
            at = pl.multiple_of(place_of(whose, j, n % RING) * ROWS, ROWS)
            copies.append(
                pltpu.make_async_copy(
                    line.at[j, pl.ds(0, matrices)], w_all.at[:, pl.ds(at, ROWS), :], w_sems.at[n * RING + j]
                )
            )
    for c in copies:
        c.start()
    for c in copies:
        c.wait()


def pair_body(*refs):
    pieces, lines = refs[:8], refs[8:16]
    near, wide, near_tail, wide_tail, x_all, w_all, x_sems, w_sems = refs[16:]
    fetch(pieces, lines, x_all, w_all, x_sems, w_sems, 2 * GROUPS)
    for role in range(2):
        for g in range(GROUPS):
            for b in range(BATCHES):
                y = jnp.dot(x_all[b], w_all[role * GROUPS + g], preferred_element_type=jnp.float32)
                y = y.astype(jnp.bfloat16)
                if g == 2:
                    wide[role, b] = y
                    wide_tail[role, b] = y[SPAN // 2 :]
                else:
                    near[g, role, b] = y
                    if g == 0:
                        near_tail[role, b, : HALOS[0]] = y[SPAN - HALOS[0] :]
                    else:
                        near_tail[role, b, HALOS[0] :] = y[SPAN - HALOS[1] :]


def project_pairs(pieces, lines):
    bf = lambda *d: jax.ShapeDtypeStruct(d, jnp.bfloat16)
    return pl.pallas_call(
        pair_body,
        out_shape=(
            bf(2, 2, BATCHES, SPAN, COLS), bf(2, BATCHES, SPAN, COLS),
            bf(2, BATCHES, HALOS[0] + HALOS[1], COLS), bf(2, BATCHES, SPAN // 2, COLS),
        ),
        in_specs=[ANY] * 16, out_specs=(VMEM,) * 4,
        scratch_shapes=[
            pltpu.VMEM((BATCHES, SPAN, WIDTH), jnp.bfloat16),
            pltpu.VMEM((2 * GROUPS, WIDTH, COLS), jnp.bfloat16),
            pltpu.SemaphoreType.DMA((8,)), pltpu.SemaphoreType.DMA((32,)),
        ],
        compiler_params=PARAMS, name="project_pairs",
    )(*pieces, *lines)


def query_body(*refs):
    pieces, lines = refs[:8], refs[8:16]
    out, x_all, w_all, x_sems, w_sems = refs[16:]
    fetch(pieces, lines, x_all, w_all, x_sems, w_sems, GROUPS)
    for g in range(GROUPS):
        for b in range(BATCHES):
            y = jnp.dot(x_all[b], w_all[g], preferred_element_type=jnp.float32)
            out[g, b] = y.astype(jnp.bfloat16)


def project_queries(pieces, lines):
    return pl.pallas_call(
        query_body,
        out_shape=jax.ShapeDtypeStruct((GROUPS, BATCHES, SPAN, COLS), jnp.bfloat16),
        in_specs=[ANY] * 16, out_specs=VMEM,
        scratch_shapes=[
            pltpu.VMEM((BATCHES, SPAN, WIDTH), jnp.bfloat16),
            pltpu.VMEM((GROUPS, WIDTH, COLS), jnp.bfloat16),
            pltpu.SemaphoreType.DMA((8,)), pltpu.SemaphoreType.DMA((32,)),
        ],
        compiler_params=PARAMS, name="project_queries",
    )(*pieces, *lines)


def bias_of(group, block):
    halo, dilation = HALOS[group], DILATIONS[group]
    dims = (BLOCK, BLOCK + halo)
    q = lax.broadcasted_iota(jnp.int32, dims, 0)
    k = lax.broadcasted_iota(jnp.int32, dims, 1)
    lag = q + halo - k
    start = (lax.axis_index("sp") // 2) * SPAN + block * BLOCK - halo
    seen = (lag >= 0) & (lag <= STEPS * dilation) & ((lag & (dilation - 1)) == 0) & (k + start >= 0)
    return jnp.where(seen, 0.0, -1e30).astype(jnp.float32)


def attend(q, k, v, bias):
    s = lax.dot_general(q, k, (((1,), (1,)), ((), ())), preferred_element_type=jnp.float32)
    s = s * (1.0 / math.sqrt(HEAD_WIDTH)) + bias
    peak = jnp.max(s, axis=-1, keepdims=True)
    lifted = jnp.exp(s - peak)
    total = jnp.sum(lifted, axis=-1, keepdims=True)
    o = jnp.dot(lifted.astype(jnp.bfloat16), v, preferred_element_type=jnp.float32)
    return o / total, peak + jnp.log(total)


def joined(o1, l1, o2, l2):
    top = jnp.maximum(l1, l2)
    a, c = jnp.exp(l1 - top), jnp.exp(l2 - top)
    total = a + c
    return (a * o1 + c * o2) / total, top + jnp.log(total)


def near_body(q, near, tail, out, logs, k0, k1, sems):
    copies = [
        pltpu.make_async_copy(tail.at[:, :, pl.ds(0, HALOS[0])], k0.at[:, :, pl.ds(0, HALOS[0])], sems.at[0]),
        pltpu.make_async_copy(tail.at[:, :, pl.ds(HALOS[0], HALOS[1])], k1.at[:, :, pl.ds(0, HALOS[1])], sems.at[1]),
        pltpu.make_async_copy(near.at[0], k0.at[:, :, pl.ds(HALOS[0], SPAN)], sems.at[2]),
        pltpu.make_async_copy(near.at[1], k1.at[:, :, pl.ds(HALOS[1], SPAN)], sems.at[3]),
    ]
    for c in copies:
        c.start()
    for c in copies:
        c.wait()
    for i in range(SPAN // BLOCK):
        rows = slice(i * BLOCK, (i + 1) * BLOCK)
        biases = [bias_of(g, i) for g in range(2)]
        for b in range(BATCHES):
            for h in range(COLS // HEAD_WIDTH):
                cols = slice(h * HEAD_WIDTH, (h + 1) * HEAD_WIDTH)
                parts = []
                for g, held in enumerate((k0, k1)):
                    keys = slice(i * BLOCK, (i + 1) * BLOCK + HALOS[g])
                    parts.append(attend(q[g, b, rows, cols], held[0, b, keys, cols], held[1, b, keys, cols], biases[g]))
                o, l = joined(*parts[0], *parts[1])
                out[b, rows, cols] = o
                logs[b, rows, cols] = jnp.broadcast_to(l, (BLOCK, HEAD_WIDTH))


def attend_near(q, near, tail):
    shape = jax.ShapeDtypeStruct((BATCHES, SPAN, COLS), jnp.float32)
    return pl.pallas_call(
        near_body, out_shape=(shape, shape), in_specs=[VMEM, ANY, ANY], out_specs=(VMEM, VMEM),
        scratch_shapes=[
            pltpu.VMEM((2, BATCHES, HALOS[0] + SPAN, COLS), jnp.bfloat16),
            pltpu.VMEM((2, BATCHES, HALOS[1] + SPAN, COLS), jnp.bfloat16),
            pltpu.SemaphoreType.DMA((4,)),
        ],
        compiler_params=PARAMS, name="attend_near",
    )(q, near, tail)


def wide_body(q, wide, back, tail, other, logs, c0, c1, c2, c3, kept, sent, held, mixed, sems):
    copies = [
        pltpu.make_async_copy(tail, held.at[:, :, pl.ds(0, SPAN // 2)], sems.at[0]),
        pltpu.make_async_copy(back, held.at[:, :, pl.ds(SPAN // 2, SPAN)], sems.at[1]),
        pltpu.make_async_copy(wide, held.at[:, :, pl.ds(HALOS[2], SPAN)], sems.at[2]),
    ]
    for c in copies:
        c.start()
    for c in copies:
        c.wait()
    core, t = lax.axis_index("sp") % 2, lax.axis_index("tp")
    for i in range(SPAN // BLOCK):
        rows = slice(i * BLOCK, (i + 1) * BLOCK)
        bias = bias_of(2, i)
        for b in range(BATCHES):
            for h in range(COLS // HEAD_WIDTH):
                cols = slice(h * HEAD_WIDTH, (h + 1) * HEAD_WIDTH)
                keys = slice(i * BLOCK, (i + 1) * BLOCK + HALOS[2])
                o, l = attend(q[2, b, rows, cols], held[0, b, keys, cols], held[1, b, keys, cols], bias)
                o, l = joined(other[b, rows, cols], logs[b, rows, cols], o, l)
                mixed[b, rows, cols] = o.astype(jnp.bfloat16)
                line = jnp.transpose(l)[0:1]

                @pl.when(core == i)
                def _():
                    kept[b * 2 + h : b * 2 + h + 1, :] = line

                @pl.when(core != i)
                def _():
                    sent[b * 2 + h : b * 2 + h + 1, :] = line

    for d, out in enumerate((c0, c1, c2, c3)):
        for far in range(2):
            whose = core if far == 0 else 1 - core
            at = pl.multiple_of(whose * (RING * PIECE) + ((t + d) % RING) * PIECE, PIECE)
            out[far] = mixed[:, pl.ds(at, PIECE), :]


def attend_wide(q, wide, back, tail, other, logs):
    piece = jax.ShapeDtypeStruct((2, BATCHES, PIECE, COLS), jnp.bfloat16)
    line = jax.ShapeDtypeStruct((2 * BATCHES, BLOCK), jnp.float32)
    return pl.pallas_call(
        wide_body, out_shape=(piece,) * 4 + (line,) * 2, in_specs=[VMEM, ANY, ANY, ANY, VMEM, VMEM],
        out_specs=(VMEM,) * 6,
        scratch_shapes=[
            pltpu.VMEM((2, BATCHES, HALOS[2] + SPAN, COLS), jnp.bfloat16),
            pltpu.VMEM((BATCHES, SPAN, COLS), jnp.bfloat16),
            pltpu.SemaphoreType.DMA((3,)),
        ],
        compiler_params=PARAMS, name="attend_wide",
    )(q, wide, back, tail, other, logs)


def lay_body(*refs):
    own, out, sems = refs[:8], refs[8], refs[9]
    core, t = lax.axis_index("sp") % 2, lax.axis_index("tp")
    copies = []
    for n, ref in enumerate(own):
        whose = core if n < RING else 1 - core
        slot = (t + RING - n % RING) % RING
        for e in range(RING):
            for j in range(RING):
                at = pl.multiple_of(place_of(whose, j, e) * ROWS, ROWS)
                copies.append(
                    pltpu.make_async_copy(ref.at[e * RING + j], out.at[slot, pl.ds(at, ROWS), :], sems.at[n, e * RING + j])
                )
    for c in copies:
        c.start()
    for c in copies:
        c.wait()


def lay_out(parts):
    return pl.pallas_call(
        lay_body, out_shape=jax.ShapeDtypeStruct((RING, WIDTH, COLS), jnp.bfloat16), in_specs=[ANY] * 8, out_specs=VMEM,
        scratch_shapes=[pltpu.SemaphoreType.DMA((8, 16))], compiler_params=PARAMS, name="lay_out",
    )(*parts)


def final_body(r0, r1, r2, r3, s0, s1, s2, s3, w, out, held):
    core, t = lax.axis_index("sp") % 2, lax.axis_index("tp")
    for d, (r, s) in enumerate(((r0, s0), (r1, s1), (r2, s2), (r3, s3))):
        slot = (t + RING - d) % RING
        held[slot, core] = r[0].reshape(BATCHES * PIECE, COLS)
        held[slot, 1 - core] = s[...].reshape(BATCHES * PIECE, COLS)
    for n in range(4):
        cols = slice(n * 512, (n + 1) * 512)
        acc = None
        for slot in range(RING):
            a = held[slot].reshape(2 * BATCHES * PIECE, COLS)
            y = lax.dot_general(a, w[slot, cols], (((1,), (1,)), ((), ())), preferred_element_type=jnp.float32)
            acc = y if acc is None else acc + y
        acc = acc.astype(jnp.bfloat16)
        for b in range(2 * BATCHES):
            out[:, b, cols] = acc[b * PIECE : (b + 1) * PIECE]


def finish(received, crossed, w):
    return pl.pallas_call(
        final_body, out_shape=jax.ShapeDtypeStruct((PIECE, 2 * BATCHES, WIDTH), jnp.bfloat16),
        in_specs=[VMEM] * 9, out_specs=VMEM,
        scratch_shapes=[pltpu.VMEM((RING, 2, BATCHES * PIECE, COLS), jnp.bfloat16)],
        compiler_params=PARAMS, name="finish",
    )(*received, *crossed, w)


def shards(tokens, norm_gain, w_query, w_key, w_value, w_out):
    keep, send = norm_rows(tokens, norm_gain)
    core = lax.axis_index("sp") % 2

    pair_lines = spread(jnp.concatenate((w_key, w_value), 0))
    pair_lines = pair_lines + [swapped(a) for a in pair_lines]

    pieces = [keep] + [turned(keep, d) for d in (1, 2, 3)]
    crossing = swapped(send)
    pieces = pieces + [crossing] + [turned(crossing, d) for d in (1, 2, 3)]

    rest = spread(jnp.concatenate((w_query, jnp.transpose(w_out)[None]), 0))
    outs = jnp.concatenate([a[:, GROUPS] for a in rest], 0)
    outs = [outs] + [turned(outs, d) for d in (1, 2, 3)]
    rest = rest + [swapped(a) for a in rest]
    outs = outs + [swapped(a) for a in outs]
    laid = lay_out(outs)

    near, wide, near_tail, wide_tail = project_pairs(pieces, pair_lines)
    near_tail = from_behind(near_tail, 1)
    wide_tail = from_behind(wide_tail, 2)
    back = from_behind(wide, 1)
    queries = project_queries(pieces, rest)
    other, logs = attend_near(queries, near, near_tail)
    *combined, kept, sent = attend_wide(queries, wide, back, wide_tail, other, logs)

    received = [combined[0]] + [turned(combined[d], d) for d in (1, 2, 3)]
    crossed = [swapped(a[1]) for a in received]
    mixed = finish(received, crossed, laid)

    came = swapped(sent)
    low = jnp.where(core == 0, kept, came)
    high = jnp.where(core == 0, came, kept)
    log_weight = jnp.concatenate((low, high), 0).reshape(2 * BATCHES, 2, BLOCK)
    return (mixed, jnp.transpose(log_weight, (2, 0, 1)))


def solution(mesh):
    in_specs = (
        P(("sp", "tp"), None, None),
        P(),
        P(None, "sp", "tp"),
        P(None, "sp", "tp"),
        P(None, "sp", "tp"),
        P("tp", "sp"),
    )
    out_specs = (P(("sp", "tp"), None, None), P("sp", None, "tp"))
    return jax.shard_map(shards, mesh=mesh, in_specs=in_specs, out_specs=out_specs, check_vma=False)
```

```python
import math

import jax
import jax.numpy as jnp
from jax import lax
from jax.experimental import pallas as pl
from jax.experimental.pallas import tpu as pltpu
from jax.sharding import PartitionSpec as P


GROUPS = 3
ORDER = (2, 0, 1)
STEPS = 24
DILATIONS = (1, 4, 16)
HALOS = (32, 96, 384)
RING = 4
BATCHES = 3
PIECE = 32
SPAN = 256
HEAD_WIDTH = 128
COLS = 256
ROWS = 64
WIDTH = 2048
BLOCK = 128

epsilon = 1e-06


def chip(z, y, core):
    return (z % RING) * 8 + (y % RING) * 2 + core


def chips():
    return [(z, y, core) for z in range(RING) for y in range(RING) for core in range(2)]


def first_leg(shift):
    return [(chip(z, y, k), chip(z + shift * k, y + shift * (1 - k), k)) for z, y, k in chips()]


def second_leg(shift):
    return [(chip(z, y, k), chip(z + shift * (1 - k), y + shift * k, k)) for z, y, k in chips()]


SWAP = [(i, i ^ 1) for i in range(32)]


def swapped(a):
    return lax.ppermute(a, "sp", SWAP)


def turned(a, shift):
    return lax.ppermute(a, "tp", [(i, (i + shift) % RING) for i in range(RING)])


def from_behind(a, blocks):
    return lax.ppermute(a, "sp", [(i, i + 2 * blocks) for i in range(32 - 2 * blocks)])


def place_of(core, first, second):
    s = lax.axis_index("sp")
    z, y = s // 8, (s // 2) % RING
    up = jnp.where(core == 0, second, first)
    along = jnp.where(core == 0, first, second)
    return ((z + RING - up) % RING) * 8 + ((y + RING - along) % RING) * 2 + core


ANY = pl.BlockSpec(memory_space=pl.ANY)
VMEM = pl.BlockSpec(memory_space=pltpu.VMEM)
PARAMS = pltpu.CompilerParams(vmem_limit_bytes=56 * 1024 * 1024)


def bf(*dims):
    return jax.ShapeDtypeStruct(dims, jnp.bfloat16)


def prepare_body(tokens, gain, w_query, w_key, w_value, keep, send, pairs, queries):
    core = lax.axis_index("sp") % 2
    widened_gain = gain[...]
    for b in range(2 * BATCHES):
        v = tokens[b].astype(jnp.float32)
        v = v * lax.rsqrt(jnp.mean(v * v, axis=-1, keepdims=True) + epsilon)
        n = (v * widened_gain).astype(jnp.bfloat16)

        @pl.when(core == b // BATCHES)
        def _():
            keep[b % BATCHES] = n

        @pl.when(core != b // BATCHES)
        def _():
            send[b % BATCHES] = n

    for place, g in enumerate(ORDER):
        pairs[2 * place] = w_key[g]
        pairs[2 * place + 1] = w_value[g]
    queries[...] = w_query[...]


def prepare(tokens, gain, w_query, w_key, w_value):
    shape = bf(BATCHES, PIECE, WIDTH)
    return pl.pallas_call(
        prepare_body, out_shape=(shape, shape, bf(2 * GROUPS, ROWS, COLS), bf(GROUPS, ROWS, COLS)),
        in_specs=[VMEM] * 5, out_specs=(VMEM,) * 4, compiler_params=PARAMS, name="prepare",
    )(jnp.transpose(tokens, (1, 0, 2)), gain.reshape(1, WIDTH), w_query, w_key, w_value)


def fetch(pieces, lines, x_all, x_sems, wanted):
    s, t = lax.axis_index("sp"), lax.axis_index("tp")
    core = s % 2
    copies = []
    for n, piece in enumerate(pieces):
        whose = core if n < RING else 1 - core
        at = whose * (RING * PIECE) + ((t + RING - n % RING) % RING) * PIECE
        at = pl.multiple_of(at, PIECE)
        copies.append(pltpu.make_async_copy(piece, x_all.at[:, pl.ds(at, PIECE), :], x_sems.at[n]))
    for n, line in enumerate(lines):
        whose = core if n < RING else 1 - core
        for j in range(RING):
            at = pl.multiple_of(place_of(whose, j, n % RING) * ROWS, ROWS)
            for first, count, w_all, w_sems in wanted:
                copies.append(
                    pltpu.make_async_copy(
                        line.at[j, pl.ds(first, count)], w_all.at[:, pl.ds(at, ROWS), :], w_sems.at[n * RING + j]
                    )
                )
    for c in copies:
        c.start()
    for c in copies:
        c.wait()


def wide_pair_body(*refs):
    pieces, lines = refs[:8], refs[8:16]
    wide, wide_tail, x_all, w_all, x_sems, w_sems = refs[16:]
    fetch(pieces, lines, x_all, x_sems, ((0, 2, w_all, w_sems),))
    for role in range(2):
        for b in range(BATCHES):
            y = jnp.dot(x_all[b], w_all[role], preferred_element_type=jnp.float32).astype(jnp.bfloat16)
            wide[role, b] = y
            wide_tail[role, b] = y[SPAN // 2 :]


def project_wide(pieces, lines):
    return pl.pallas_call(
        wide_pair_body,
        out_shape=(bf(2, BATCHES, SPAN, COLS), bf(2, BATCHES, SPAN // 2, COLS)),
        in_specs=[ANY] * 16, out_specs=(VMEM,) * 2,
        scratch_shapes=[
            pltpu.VMEM((BATCHES, SPAN, WIDTH), jnp.bfloat16), pltpu.VMEM((2, WIDTH, COLS), jnp.bfloat16),
            pltpu.SemaphoreType.DMA((8,)), pltpu.SemaphoreType.DMA((32,)),
        ],
        compiler_params=PARAMS, name="project_wide",
    )(*pieces, *lines)


def near_pair_body(*refs):
    pieces, lines = refs[:8], refs[8:16]
    near, near_tail, x_all, w_all, x_sems, w_sems = refs[16:]
    fetch(pieces, lines, x_all, x_sems, ((2, 4, w_all, w_sems),))
    for g in range(2):
        for role in range(2):
            for b in range(BATCHES):
                y = jnp.dot(x_all[b], w_all[2 * g + role], preferred_element_type=jnp.float32).astype(jnp.bfloat16)
                near[g, role, b] = y
                if g == 0:
                    near_tail[role, b, : HALOS[0]] = y[SPAN - HALOS[0] :]
                else:
                    near_tail[role, b, HALOS[0] :] = y[SPAN - HALOS[1] :]


def project_near(pieces, lines):
    return pl.pallas_call(
        near_pair_body,
        out_shape=(bf(2, 2, BATCHES, SPAN, COLS), bf(2, BATCHES, HALOS[0] + HALOS[1], COLS)),
        in_specs=[ANY] * 16, out_specs=(VMEM,) * 2,
        scratch_shapes=[
            pltpu.VMEM((BATCHES, SPAN, WIDTH), jnp.bfloat16), pltpu.VMEM((4, WIDTH, COLS), jnp.bfloat16),
            pltpu.SemaphoreType.DMA((8,)), pltpu.SemaphoreType.DMA((32,)),
        ],
        compiler_params=PARAMS, name="project_near",
    )(*pieces, *lines)


def query_body(*refs):
    pieces, lines = refs[:8], refs[8:16]
    out, laid, x_all, w_all, x_sems, w_sems, o_sems = refs[16:]
    fetch(pieces, lines, x_all, x_sems, ((0, GROUPS, w_all, w_sems), (GROUPS, RING, laid, o_sems)))
    for g in range(GROUPS):
        for b in range(BATCHES):
            y = jnp.dot(x_all[b], w_all[g], preferred_element_type=jnp.float32)
            out[g, b] = y.astype(jnp.bfloat16)


def project_queries(pieces, lines):
    return pl.pallas_call(
        query_body,
        out_shape=(bf(GROUPS, BATCHES, SPAN, COLS), bf(RING, WIDTH, COLS)),
        in_specs=[ANY] * 16, out_specs=(VMEM,) * 2,
        scratch_shapes=[
            pltpu.VMEM((BATCHES, SPAN, WIDTH), jnp.bfloat16), pltpu.VMEM((GROUPS, WIDTH, COLS), jnp.bfloat16),
            pltpu.SemaphoreType.DMA((8,)), pltpu.SemaphoreType.DMA((32,)), pltpu.SemaphoreType.DMA((32,)),
        ],
        compiler_params=PARAMS, name="project_queries",
    )(*pieces, *lines)


def bias_of(group, block):
    halo, dilation = HALOS[group], DILATIONS[group]
    dims = (BLOCK, BLOCK + halo)
    q = lax.broadcasted_iota(jnp.int32, dims, 0)
    k = lax.broadcasted_iota(jnp.int32, dims, 1)
    lag = q + halo - k
    start = (lax.axis_index("sp") // 2) * SPAN + block * BLOCK - halo
    seen = (lag >= 0) & (lag <= STEPS * dilation) & ((lag & (dilation - 1)) == 0) & (k + start >= 0)
    return jnp.where(seen, 0.0, -1e30).astype(jnp.float32)


def attend(q, k, v, bias):
    s = lax.dot_general(q, k, (((1,), (1,)), ((), ())), preferred_element_type=jnp.float32)
    s = s * (1.0 / math.sqrt(HEAD_WIDTH)) + bias
    peak = jnp.max(s, axis=-1, keepdims=True)
    lifted = jnp.exp(s - peak)
    total = jnp.sum(lifted, axis=-1, keepdims=True)
    o = jnp.dot(lifted.astype(jnp.bfloat16), v, preferred_element_type=jnp.float32)
    return o / total, peak + jnp.log(total)


def joined(o1, l1, o2, l2):
    top = jnp.maximum(l1, l2)
    a, c = jnp.exp(l1 - top), jnp.exp(l2 - top)
    total = a + c
    return (a * o1 + c * o2) / total, top + jnp.log(total)


def near_body(q, near, tail, out, logs, k0, k1, sems):
    copies = [
        pltpu.make_async_copy(tail.at[:, :, pl.ds(0, HALOS[0])], k0.at[:, :, pl.ds(0, HALOS[0])], sems.at[0]),
        pltpu.make_async_copy(tail.at[:, :, pl.ds(HALOS[0], HALOS[1])], k1.at[:, :, pl.ds(0, HALOS[1])], sems.at[1]),
        pltpu.make_async_copy(near.at[0], k0.at[:, :, pl.ds(HALOS[0], SPAN)], sems.at[2]),
        pltpu.make_async_copy(near.at[1], k1.at[:, :, pl.ds(HALOS[1], SPAN)], sems.at[3]),
    ]
    for c in copies:
        c.start()
    for c in copies:
        c.wait()
    for i in range(SPAN // BLOCK):
        rows = slice(i * BLOCK, (i + 1) * BLOCK)
        biases = [bias_of(g, i) for g in range(2)]
        for b in range(BATCHES):
            for h in range(COLS // HEAD_WIDTH):
                cols = slice(h * HEAD_WIDTH, (h + 1) * HEAD_WIDTH)
                parts = []
                for g, held in enumerate((k0, k1)):
                    keys = slice(i * BLOCK, (i + 1) * BLOCK + HALOS[g])
                    parts.append(attend(q[g, b, rows, cols], held[0, b, keys, cols], held[1, b, keys, cols], biases[g]))
                o, l = joined(*parts[0], *parts[1])
                out[b, rows, cols] = o
                logs[b, rows, cols] = jnp.broadcast_to(l, (BLOCK, HEAD_WIDTH))


def attend_near(q, near, tail):
    shape = jax.ShapeDtypeStruct((BATCHES, SPAN, COLS), jnp.float32)
    return pl.pallas_call(
        near_body, out_shape=(shape, shape), in_specs=[VMEM, ANY, ANY], out_specs=(VMEM, VMEM),
        scratch_shapes=[
            pltpu.VMEM((2, BATCHES, HALOS[0] + SPAN, COLS), jnp.bfloat16),
            pltpu.VMEM((2, BATCHES, HALOS[1] + SPAN, COLS), jnp.bfloat16),
            pltpu.SemaphoreType.DMA((4,)),
        ],
        compiler_params=PARAMS, name="attend_near",
    )(q, near, tail)


def wide_body(q, wide, back, tail, other, logs, c0, c1, c2, c3, kept, sent, held, mixed, sems):
    copies = [
        pltpu.make_async_copy(tail, held.at[:, :, pl.ds(0, SPAN // 2)], sems.at[0]),
        pltpu.make_async_copy(back, held.at[:, :, pl.ds(SPAN // 2, SPAN)], sems.at[1]),
        pltpu.make_async_copy(wide, held.at[:, :, pl.ds(HALOS[2], SPAN)], sems.at[2]),
    ]
    for c in copies:
        c.start()
    for c in copies:
        c.wait()
    core, t = lax.axis_index("sp") % 2, lax.axis_index("tp")
    for i in range(SPAN // BLOCK):
        rows = slice(i * BLOCK, (i + 1) * BLOCK)
        bias = bias_of(2, i)
        for b in range(BATCHES):
            for h in range(COLS // HEAD_WIDTH):
                cols = slice(h * HEAD_WIDTH, (h + 1) * HEAD_WIDTH)
                keys = slice(i * BLOCK, (i + 1) * BLOCK + HALOS[2])
                o, l = attend(q[2, b, rows, cols], held[0, b, keys, cols], held[1, b, keys, cols], bias)
                o, l = joined(other[b, rows, cols], logs[b, rows, cols], o, l)
                mixed[b, rows, cols] = o.astype(jnp.bfloat16)
                line = jnp.transpose(l)[0:1]

                @pl.when(core == i)
                def _():
                    kept[b * 2 + h : b * 2 + h + 1, :] = line

                @pl.when(core != i)
                def _():
                    sent[b * 2 + h : b * 2 + h + 1, :] = line

    for d, out in enumerate((c0, c1, c2, c3)):
        for far in range(2):
            whose = core if far == 0 else 1 - core
            at = pl.multiple_of(whose * (RING * PIECE) + ((t + d) % RING) * PIECE, PIECE)
            out[far] = mixed[:, pl.ds(at, PIECE), :]


def attend_wide(q, wide, back, tail, other, logs):
    piece = jax.ShapeDtypeStruct((2, BATCHES, PIECE, COLS), jnp.bfloat16)
    line = jax.ShapeDtypeStruct((2 * BATCHES, BLOCK), jnp.float32)
    return pl.pallas_call(
        wide_body, out_shape=(piece,) * 4 + (line,) * 2, in_specs=[VMEM, ANY, ANY, ANY, VMEM, VMEM],
        out_specs=(VMEM,) * 6,
        scratch_shapes=[
            pltpu.VMEM((2, BATCHES, HALOS[2] + SPAN, COLS), jnp.bfloat16),
            pltpu.VMEM((BATCHES, SPAN, COLS), jnp.bfloat16),
            pltpu.SemaphoreType.DMA((3,)),
        ],
        compiler_params=PARAMS, name="attend_wide",
    )(q, wide, back, tail, other, logs)


def final_body(r0, r1, r2, r3, s0, s1, s2, s3, w, out, held):
    core = lax.axis_index("sp") % 2
    for d, (r, s) in enumerate(((r0, s0), (r1, s1), (r2, s2), (r3, s3))):
        held[d, core] = r[0].reshape(BATCHES * PIECE, COLS)
        held[d, 1 - core] = s[...].reshape(BATCHES * PIECE, COLS)
    for n in range(4):
        cols = slice(n * 512, (n + 1) * 512)
        acc = None
        for d in range(RING):
            a = held[d].reshape(2 * BATCHES * PIECE, COLS)
            y = lax.dot_general(a, w[d, cols], (((1,), (1,)), ((), ())), preferred_element_type=jnp.float32)
            acc = y if acc is None else acc + y
        acc = acc.astype(jnp.bfloat16)
        for b in range(2 * BATCHES):
            out[b, :, cols] = acc[b * PIECE : (b + 1) * PIECE]


def finish(received, crossed, w):
    mixed = pl.pallas_call(
        final_body, out_shape=bf(2 * BATCHES, PIECE, WIDTH),
        in_specs=[VMEM] * 9, out_specs=VMEM,
        scratch_shapes=[pltpu.VMEM((RING, 2, BATCHES * PIECE, COLS), jnp.bfloat16)],
        compiler_params=PARAMS, name="finish",
    )(*received, *crossed, w)
    return jnp.transpose(mixed, (1, 0, 2))


def ring_of(a):
    came = {d: turned(a, d) for d in (1, 3, 2)}
    return [a, came[1], came[2], came[3]]


def spread(own):
    near = {d: lax.ppermute(own, "sp", first_leg(d)) for d in (1, 3, 2)}
    line = jnp.stack((own, near[1], near[2], near[3]))
    far = {d: lax.ppermute(line, "sp", second_leg(d)) for d in (1, 3, 2)}
    lines = [line, far[1], far[2], far[3]]
    return lines + [swapped(a) for a in lines]


def layer(tokens, norm_gain, w_query, w_key, w_value, w_out):
    core = lax.axis_index("sp") % 2
    keep, send, pair_own, query_own = prepare(tokens, norm_gain, w_query, w_key, w_value)
    crossing = swapped(send)
    pieces = ring_of(keep) + ring_of(crossing)
    pair_lines = spread(pair_own)
    outs = ring_of(jnp.transpose(w_out))
    rest = spread(jnp.concatenate((query_own, jnp.stack(outs)), 0))

    wide, wide_tail = project_wide(pieces, pair_lines)
    back = from_behind(wide, 1)
    wide_tail = from_behind(wide_tail, 2)
    near, near_tail = project_near(pieces, pair_lines)
    near_tail = from_behind(near_tail, 1)
    queries, laid = project_queries(pieces, rest)
    other, logs = attend_near(queries, near, near_tail)
    *combined, kept, sent = attend_wide(queries, wide, back, wide_tail, other, logs)

    received = [combined[0]] + [turned(combined[d], d) for d in (1, 2, 3)]
    crossed = [swapped(a[1]) for a in received]
    mixed = finish(received, crossed, laid)

    came = swapped(sent)
    low = jnp.where(core == 0, kept, came)
    high = jnp.where(core == 0, came, kept)
    log_weight = jnp.concatenate((low, high), 0).reshape(2 * BATCHES, 2, BLOCK)
    return (mixed, jnp.transpose(log_weight, (2, 0, 1)))


def solution(mesh):
    in_specs = (
        P(("sp", "tp"), None, None),
        P(),
        P(None, "sp", "tp"),
        P(None, "sp", "tp"),
        P(None, "sp", "tp"),
        P("tp", "sp"),
    )
    out_specs = (P(("sp", "tp"), None, None), P("sp", None, "tp"))
    return jax.shard_map(layer, mesh=mesh, in_specs=in_specs, out_specs=out_specs, check_vma=False)
```

```python
import math

import jax
import jax.numpy as jnp
from jax import lax
from jax.experimental import pallas as pl
from jax.experimental.pallas import tpu as pltpu
from jax.sharding import PartitionSpec as P


GROUPS = 3
STEPS = 24
DILATIONS = (1, 4, 16)
HALOS = (32, 96, 384)
RING = 4
BATCHES = 3
PIECE = 32
SPAN = 256
HEAD_WIDTH = 128
COLS = 256
ROWS = 64
WIDTH = 2048
BLOCK = 128

epsilon = 1e-06


def chip(z, y, core):
    return (z % RING) * 8 + (y % RING) * 2 + core


def chips():
    return [(z, y, core) for z in range(RING) for y in range(RING) for core in range(2)]


def first_leg(shift, kind):
    def way(k):
        return k if kind == 0 else 0

    return [(chip(z, y, k), chip(z + shift * way(k), y + shift * (1 - way(k)), k)) for z, y, k in chips()]


def second_leg(shift, kind):
    def way(k):
        return k if kind == 0 else 0

    return [(chip(z, y, k), chip(z + shift * (1 - way(k)), y + shift * way(k), k)) for z, y, k in chips()]


SWAP = [(i, i ^ 1) for i in range(32)]


def swapped(a):
    return lax.ppermute(a, "sp", SWAP)


def turned(a, shift):
    return lax.ppermute(a, "tp", [(i, (i + shift) % RING) for i in range(RING)])


def from_behind(a, blocks):
    return lax.ppermute(a, "sp", [(i, i + 2 * blocks) for i in range(32 - 2 * blocks)])


def place_of(core, first, second, kind):
    s = lax.axis_index("sp")
    z, y = s // 8, (s // 2) % RING
    if kind == 0:
        up = jnp.where(core == 0, second, first)
        along = jnp.where(core == 0, first, second)
    else:
        up, along = second, first
    return ((z + RING - up) % RING) * 8 + ((y + RING - along) % RING) * 2 + core


ANY = pl.BlockSpec(memory_space=pl.ANY)
VMEM = pl.BlockSpec(memory_space=pltpu.VMEM)
PARAMS = pltpu.CompilerParams(vmem_limit_bytes=56 * 1024 * 1024)
HALF = SPAN // 2
NEAR = 4


def bf(*dims):
    return jax.ShapeDtypeStruct(dims, jnp.bfloat16)


def pack_body(w_query, w_key, w_value, wide, rest):
    wide[0] = w_key[2]
    wide[1] = w_value[2]
    for g in range(2):
        rest[2 * g] = w_key[g]
        rest[2 * g + 1] = w_value[g]
    rest[NEAR:] = w_query[...]


def pack(w_query, w_key, w_value):
    return pl.pallas_call(
        pack_body, out_shape=(bf(2, ROWS, COLS), bf(NEAR + GROUPS, ROWS, COLS)),
        in_specs=[VMEM] * 3, out_specs=(VMEM,) * 2, compiler_params=PARAMS, name="pack",
    )(w_query, w_key, w_value)


def norm_body(tokens, other, gain, late, early):
    core = lax.axis_index("sp") % 2
    widened_gain = gain[...]

    def normed(v):
        v = v.astype(jnp.float32)
        v = v * lax.rsqrt(jnp.mean(v * v, axis=-1, keepdims=True) + epsilon)
        return (v * widened_gain).astype(jnp.bfloat16)

    for b in range(BATCHES):
        mine = normed(tokens[core * BATCHES + b])
        theirs = normed(other[b])

        @pl.when(core == 1)
        def _():
            late[b] = mine
            early[b] = theirs

        @pl.when(core == 0)
        def _():
            late[b] = theirs
            early[b] = mine


def norm_rows(tokens, other, gain):
    shape = bf(BATCHES, PIECE, WIDTH)
    return pl.pallas_call(
        norm_body, out_shape=(shape, shape), in_specs=[VMEM] * 3, out_specs=(VMEM,) * 2,
        compiler_params=PARAMS, name="norm_rows",
    )(tokens, other, gain.reshape(1, WIDTH))


def row_copies(pieces, base, x_all, sems):
    t = lax.axis_index("tp")
    copies = []
    for d, piece in enumerate(pieces):
        at = pl.multiple_of(base + ((t + RING - d) % RING) * PIECE, PIECE)
        copies.append(pltpu.make_async_copy(piece, x_all.at[:, pl.ds(at, PIECE), :], sems.at[base // HALF, d]))
    return copies


def shard_copies(lines, first, count, w_all, sems, kind):
    core = lax.axis_index("sp") % 2
    copies = []
    for n, line in enumerate(lines):
        whose = core if n < RING else 1 - core
        for j in range(RING):
            at = pl.multiple_of(place_of(whose, j, n % RING, kind) * ROWS, ROWS)
            copies.append(
                pltpu.make_async_copy(
                    line.at[j, pl.ds(first, count)], w_all.at[pl.ds(first, count), pl.ds(at, ROWS), :],
                    sems.at[n * RING + j],
                )
            )
    return copies


def wide_pair_body(*refs):
    pieces, lines = refs[:4], refs[4:12]
    out, x_all, w_all, x_sems, k_sems, v_sems = refs[12:]
    groups = [row_copies(pieces, 0, x_all, x_sems)]
    groups += [shard_copies(lines, 0, 1, w_all, k_sems, 0), shard_copies(lines, 1, 1, w_all, v_sems, 0)]
    for group in groups:
        for c in group:
            c.start()
    for c in groups[0]:
        c.wait()
    for role in range(2):
        for c in groups[1 + role]:
            c.wait()
        x = x_all[...].reshape(BATCHES * HALF, WIDTH)
        y = jnp.dot(x, w_all[role], preferred_element_type=jnp.float32)
        out[role] = y.astype(jnp.bfloat16).reshape(BATCHES, HALF, COLS)


def project_wide(pieces, lines):
    return pl.pallas_call(
        wide_pair_body, out_shape=bf(2, BATCHES, HALF, COLS), in_specs=[ANY] * 12, out_specs=VMEM,
        scratch_shapes=[
            pltpu.VMEM((BATCHES, HALF, WIDTH), jnp.bfloat16), pltpu.VMEM((2, WIDTH, COLS), jnp.bfloat16),
            pltpu.SemaphoreType.DMA((1, RING)), pltpu.SemaphoreType.DMA((32,)), pltpu.SemaphoreType.DMA((32,)),
        ],
        compiler_params=PARAMS, name="project_wide",
    )(*pieces, *lines)


def rest_body(*refs):
    early, late, lines = refs[:4], refs[4:8], refs[8:16]
    near, near_tail, queries, x_all, w_all, x_sems, a_sems, b_sems, c_sems = refs[16:]
    rows = row_copies(early, 0, x_all, x_sems) + row_copies(late, HALF, x_all, x_sems)
    groups = {
        0: rows + shard_copies(lines, 0, 1, w_all, a_sems, 0),
        1: shard_copies(lines, 1, 3, w_all, b_sems, 0),
        4: shard_copies(lines, 4, 3, w_all, c_sems, 0),
    }
    for group in groups.values():
        for c in group:
            c.start()
    for m in range(NEAR + GROUPS):
        for c in groups.get(m, ()):
            c.wait()
        x = x_all[...].reshape(BATCHES * SPAN, WIDTH)
        y = jnp.dot(x, w_all[m], preferred_element_type=jnp.float32)
        y = y.astype(jnp.bfloat16).reshape(BATCHES, SPAN, COLS)
        if m >= NEAR:
            queries[m - NEAR] = y
        else:
            near[m // 2, m % 2] = y
            if m < 2:
                near_tail[m % 2, :, : HALOS[0]] = y[:, SPAN - HALOS[0] :]
            else:
                near_tail[m % 2, :, HALOS[0] :] = y[:, SPAN - HALOS[1] :]


def project_rest(early, late, lines):
    return pl.pallas_call(
        rest_body,
        out_shape=(
            bf(2, 2, BATCHES, SPAN, COLS), bf(2, BATCHES, HALOS[0] + HALOS[1], COLS), bf(GROUPS, BATCHES, SPAN, COLS)
        ),
        in_specs=[ANY] * 16, out_specs=(VMEM,) * 3,
        scratch_shapes=[
            pltpu.VMEM((BATCHES, SPAN, WIDTH), jnp.bfloat16), pltpu.VMEM((NEAR + GROUPS, WIDTH, COLS), jnp.bfloat16),
            pltpu.SemaphoreType.DMA((2, RING)), pltpu.SemaphoreType.DMA((32,)), pltpu.SemaphoreType.DMA((32,)),
            pltpu.SemaphoreType.DMA((32,)),
        ],
        compiler_params=PARAMS, name="project_rest",
    )(*early, *late, *lines)


def bias_of(group, block):
    halo, dilation = HALOS[group], DILATIONS[group]
    dims = (BLOCK, BLOCK + halo)
    q = lax.broadcasted_iota(jnp.int32, dims, 0)
    k = lax.broadcasted_iota(jnp.int32, dims, 1)
    lag = q + halo - k
    start = (lax.axis_index("sp") // 2) * SPAN + block * BLOCK - halo
    seen = (lag >= 0) & (lag <= STEPS * dilation) & ((lag & (dilation - 1)) == 0) & (k + start >= 0)
    return jnp.where(seen, 0.0, -1e30).astype(jnp.float32)


def attend(items):
    scores = [
        lax.dot_general(q, k, (((1,), (1,)), ((), ())), preferred_element_type=jnp.float32) for q, k, _, _ in items
    ]
    lifts = []
    for s, (_, _, _, bias) in zip(scores, items):
        s = s * (1.0 / math.sqrt(HEAD_WIDTH)) + bias
        peak = jnp.max(s, axis=-1, keepdims=True)
        lifted = jnp.exp(s - peak)
        lifts.append((lifted.astype(jnp.bfloat16), peak, jnp.sum(lifted, axis=-1, keepdims=True)))
    outs = [jnp.dot(p, v, preferred_element_type=jnp.float32) for (p, _, _), (_, _, v, _) in zip(lifts, items)]
    return [(o / total, peak + jnp.log(total)) for o, (_, peak, total) in zip(outs, lifts)]


def joined(o1, l1, o2, l2):
    top = jnp.maximum(l1, l2)
    a, c = jnp.exp(l1 - top), jnp.exp(l2 - top)
    total = a + c
    return (a * o1 + c * o2) / total, top + jnp.log(total)


PLACES = [
    (b, h, slice(h * HEAD_WIDTH, (h + 1) * HEAD_WIDTH)) for b in range(BATCHES) for h in range(COLS // HEAD_WIDTH)
]


def wide_body(q, early, late, back_early, back_late, far_late, out, logs, held, sems):
    copies = [
        pltpu.make_async_copy(part, held.at[:, :, pl.ds(n * HALF, HALF)], sems.at[n])
        for n, part in enumerate((far_late, back_early, back_late, early, late))
    ]
    for c in copies:
        c.start()
    for c in copies:
        c.wait()
    for i in range(SPAN // BLOCK):
        rows = slice(i * BLOCK, (i + 1) * BLOCK)
        keys = slice(i * BLOCK, (i + 1) * BLOCK + HALOS[2])
        bias = bias_of(2, i)
        found = attend([(q[b, rows, cols], held[0, b, keys, cols], held[1, b, keys, cols], bias) for b, _, cols in PLACES])
        for (b, _, cols), (o, l) in zip(PLACES, found):
            out[b, rows, cols] = o
            logs[b, rows, cols] = jnp.broadcast_to(l, (BLOCK, HEAD_WIDTH))


def attend_wide(q, early, late, back_early, back_late, far_late):
    shape = jax.ShapeDtypeStruct((BATCHES, SPAN, COLS), jnp.float32)
    return pl.pallas_call(
        wide_body, out_shape=(shape, shape),
        in_specs=[pl.BlockSpec((pl.squeezed, BATCHES, SPAN, COLS), lambda i: (2, 0, 0, 0))] + [ANY] * 5,
        out_specs=(VMEM,) * 2, grid=(1,),
        scratch_shapes=[
            pltpu.VMEM((2, BATCHES, HALOS[2] + SPAN, COLS), jnp.bfloat16), pltpu.SemaphoreType.DMA((5,)),
        ],
        compiler_params=PARAMS, name="attend_wide",
    )(q, early, late, back_early, back_late, far_late)


def near_body(q, near, tail, other, logs, c0, c1, c2, c3, kept, sent, k0, k1, mixed, weights, sems):
    copies = [
        pltpu.make_async_copy(tail.at[:, :, pl.ds(0, HALOS[0])], k0.at[:, :, pl.ds(0, HALOS[0])], sems.at[0]),
        pltpu.make_async_copy(tail.at[:, :, pl.ds(HALOS[0], HALOS[1])], k1.at[:, :, pl.ds(0, HALOS[1])], sems.at[1]),
        pltpu.make_async_copy(near.at[0], k0.at[:, :, pl.ds(HALOS[0], SPAN)], sems.at[2]),
        pltpu.make_async_copy(near.at[1], k1.at[:, :, pl.ds(HALOS[1], SPAN)], sems.at[3]),
    ]
    for c in copies:
        c.start()
    for c in copies:
        c.wait()
    core, t = lax.axis_index("sp") % 2, lax.axis_index("tp")
    for i in range(SPAN // BLOCK):
        rows = slice(i * BLOCK, (i + 1) * BLOCK)
        biases = [bias_of(g, i) for g in range(2)]
        for some in (PLACES[:3], PLACES[3:]):
            items = []
            for g, held in enumerate((k0, k1)):
                keys = slice(i * BLOCK, (i + 1) * BLOCK + HALOS[g])
                items += [
                    (q[g, b, rows, cols], held[0, b, keys, cols], held[1, b, keys, cols], biases[g]) for b, _, cols in some
                ]
            found = attend(items)
            for n, (b, h, cols) in enumerate(some):
                o, l = joined(*found[n], *found[n + 3])
                o, l = joined(o, l, other[b, rows, cols], logs[b, rows, cols])
                mixed[b, rows, cols] = o.astype(jnp.bfloat16)
                weights[i, 2 * b + h : 2 * b + h + 1, :] = jnp.transpose(l)[0:1]
    kept[...] = weights[core]
    sent[...] = weights[1 - core]
    for d, out in enumerate((c0, c1, c2, c3)):
        for far in range(2):
            whose = core if far == 0 else 1 - core
            at = pl.multiple_of(whose * HALF + ((t + d) % RING) * PIECE, PIECE)
            out[far] = mixed[:, pl.ds(at, PIECE), :]


def attend_near(q, near, tail, other, logs):
    piece = bf(2, BATCHES, PIECE, COLS)
    line = jax.ShapeDtypeStruct((2 * BATCHES, BLOCK), jnp.float32)
    return pl.pallas_call(
        near_body, out_shape=(piece,) * 4 + (line,) * 2, grid=(1,),
        in_specs=[pl.BlockSpec((2, BATCHES, SPAN, COLS), lambda i: (0, 0, 0, 0)), ANY, ANY, VMEM, VMEM],
        out_specs=(VMEM,) * 6,
        scratch_shapes=[
            pltpu.VMEM((2, BATCHES, HALOS[0] + SPAN, COLS), jnp.bfloat16),
            pltpu.VMEM((2, BATCHES, HALOS[1] + SPAN, COLS), jnp.bfloat16),
            pltpu.VMEM((BATCHES, SPAN, COLS), jnp.bfloat16),
            pltpu.VMEM((2, 2 * BATCHES, BLOCK), jnp.float32),
            pltpu.SemaphoreType.DMA((4,)),
        ],
        compiler_params=PARAMS, name="attend_near",
    )(q, near, tail, other, logs)


def lay_body(*refs):
    lines, out, sems = refs[:8], refs[8], refs[9]
    copies = shard_copies(lines, 0, RING, out, sems, 1)
    for c in copies:
        c.start()
    for c in copies:
        c.wait()


def lay_out(lines):
    return pl.pallas_call(
        lay_body, out_shape=bf(RING, WIDTH, COLS), in_specs=[ANY] * 8, out_specs=VMEM,
        scratch_shapes=[pltpu.SemaphoreType.DMA((32,))], compiler_params=PARAMS, name="lay_out",
    )(*lines)


def final_body(r0, r1, r2, r3, s0, s1, s2, s3, w, out, held, w_all, sems):
    core = lax.axis_index("sp") % 2
    part = WIDTH // RING
    copies = [
        pltpu.make_async_copy(w.at[:, pl.ds(n * part, part)], w_all.at[n], sems.at[n]) for n in range(RING)
    ]
    for c in copies:
        c.start()
    for d, (r, s) in enumerate(((r0, s0), (r1, s1), (r2, s2), (r3, s3))):
        held[d, core] = r[0].reshape(BATCHES * PIECE, COLS)
        held[d, 1 - core] = s[...].reshape(BATCHES * PIECE, COLS)
    for n in range(RING):
        cols = slice(n * part, (n + 1) * part)
        copies[n].wait()
        acc = None
        for d in range(RING):
            a = held[d].reshape(2 * BATCHES * PIECE, COLS)
            y = lax.dot_general(a, w_all[n, d], (((1,), (1,)), ((), ())), preferred_element_type=jnp.float32)
            acc = y if acc is None else acc + y
        out[:, :, cols] = acc.astype(jnp.bfloat16).reshape(2 * BATCHES, PIECE, part)


def finish(received, crossed, w):
    mixed = pl.pallas_call(
        final_body, out_shape=bf(2 * BATCHES, PIECE, WIDTH),
        in_specs=[VMEM] * 8 + [ANY], out_specs=VMEM,
        scratch_shapes=[
            pltpu.VMEM((RING, 2, BATCHES * PIECE, COLS), jnp.bfloat16),
            pltpu.VMEM((RING, RING, WIDTH // RING, COLS), jnp.bfloat16),
            pltpu.SemaphoreType.DMA((RING,)),
        ],
        compiler_params=PARAMS, name="finish",
    )(*received, *crossed, w)
    return jnp.transpose(mixed, (1, 0, 2))


def ring_of(a):
    came = {d: turned(a, d) for d in (1, 3, 2)}
    return [a, came[1], came[2], came[3]]


def spread(own, kind):
    near = {d: lax.ppermute(own, "sp", first_leg(d, kind)) for d in (1, 3, 2)}
    line = jnp.stack((own, near[1], near[2], near[3]))
    far = {d: lax.ppermute(line, "sp", second_leg(d, kind)) for d in (1, 3, 2)}
    lines = [line, far[1], far[2], far[3]]
    return lines + [swapped(a) for a in lines]


def layer(tokens, norm_gain, w_query, w_key, w_value, w_out):
    core = lax.axis_index("sp") % 2
    tokens = jnp.transpose(tokens, (1, 0, 2))
    send = lax.dynamic_slice_in_dim(tokens, (1 - core) * BATCHES, BATCHES, 0)
    other = swapped(send)
    wide_own, rest_own = pack(w_query, w_key, w_value)
    wide_lines = spread(wide_own, 0)
    late, early = norm_rows(tokens, other, norm_gain)
    late, early = ring_of(late), ring_of(early)
    rest_lines = spread(rest_own, 0)
    out_lines = spread(jnp.stack(ring_of(jnp.transpose(w_out))), 1)

    wide_late = project_wide(late, wide_lines)
    far_late = from_behind(wide_late, 2)
    back_late = from_behind(wide_late, 1)
    wide_early = project_wide(early, wide_lines)
    back_early = from_behind(wide_early, 1)
    near, near_tail, queries = project_rest(early, late, rest_lines)
    near_tail = from_behind(near_tail, 1)
    laid = lay_out(out_lines)
    wide_out, wide_logs = attend_wide(queries, wide_early, wide_late, back_early, back_late, far_late)
    *combined, kept, sent = attend_near(queries, near, near_tail, wide_out, wide_logs)

    received = [combined[0]] + [turned(combined[d], d) for d in (1, 2, 3)]
    crossed = [swapped(a[1]) for a in received]
    mixed = finish(received, crossed, laid)

    came = swapped(sent)
    low = jnp.where(core == 0, kept, came)
    high = jnp.where(core == 0, came, kept)
    log_weight = jnp.concatenate((low, high), 0).reshape(2 * BATCHES, 2, BLOCK)
    return (mixed, jnp.transpose(log_weight, (2, 0, 1)))


def solution(mesh):
    in_specs = (
        P(("sp", "tp"), None, None),
        P(),
        P(None, "sp", "tp"),
        P(None, "sp", "tp"),
        P(None, "sp", "tp"),
        P("tp", "sp"),
    )
    out_specs = (P(("sp", "tp"), None, None), P("sp", None, "tp"))
    return jax.shard_map(layer, mesh=mesh, in_specs=in_specs, out_specs=out_specs, check_vma=False)
```

```python
import math

import jax
import jax.numpy as jnp
from jax import lax
from jax.experimental import pallas as pl
from jax.experimental.pallas import tpu as pltpu
from jax.sharding import PartitionSpec as P


GROUPS = 3
STEPS = 24
DILATIONS = (1, 4, 16)
HALOS = (32, 96, 384)
RING = 4
BATCHES = 3
PIECE = 32
SPAN = 256
HEAD_WIDTH = 128
COLS = 256
ROWS = 64
WIDTH = 2048
BLOCK = 128

epsilon = 1e-06


def chip(z, y, core):
    return (z % RING) * 8 + (y % RING) * 2 + core


def chips():
    return [(z, y, core) for z in range(RING) for y in range(RING) for core in range(2)]


def first_leg(shift, kind):
    def way(k):
        return k if kind == 0 else 0

    return [(chip(z, y, k), chip(z + shift * way(k), y + shift * (1 - way(k)), k)) for z, y, k in chips()]


def second_leg(shift, kind):
    def way(k):
        return k if kind == 0 else 0

    return [(chip(z, y, k), chip(z + shift * (1 - way(k)), y + shift * way(k), k)) for z, y, k in chips()]


SWAP = [(i, i ^ 1) for i in range(32)]


def swapped(a):
    return lax.ppermute(a, "sp", SWAP)


def turned(a, shift):
    return lax.ppermute(a, "tp", [(i, (i + shift) % RING) for i in range(RING)])


def from_behind(a, blocks):
    return lax.ppermute(a, "sp", [(i, i + 2 * blocks) for i in range(32 - 2 * blocks)])


def place_of(core, first, second, kind):
    s = lax.axis_index("sp")
    z, y = s // 8, (s // 2) % RING
    if kind == 0:
        up = jnp.where(core == 0, second, first)
        along = jnp.where(core == 0, first, second)
    else:
        up, along = second, first
    return ((z + RING - up) % RING) * 8 + ((y + RING - along) % RING) * 2 + core


ANY = pl.BlockSpec(memory_space=pl.ANY)
VMEM = pl.BlockSpec(memory_space=pltpu.VMEM)
PARAMS = pltpu.CompilerParams(vmem_limit_bytes=56 * 1024 * 1024)
HALF = SPAN // 2
NEAR = 4


def bf(*dims):
    return jax.ShapeDtypeStruct(dims, jnp.bfloat16)


def pack_body(w_query, w_key, w_value, wide, rest):
    wide[0] = w_key[2]
    wide[1] = w_value[2]
    for g in range(2):
        rest[2 * g] = w_key[g]
        rest[2 * g + 1] = w_value[g]
    rest[NEAR:] = w_query[...]


def pack(w_query, w_key, w_value):
    return pl.pallas_call(
        pack_body, out_shape=(bf(2, ROWS, COLS), bf(NEAR + GROUPS, ROWS, COLS)),
        in_specs=[VMEM] * 3, out_specs=(VMEM,) * 2, compiler_params=PARAMS, name="pack",
    )(w_query, w_key, w_value)


def norm_body(tokens, other, gain, late, early):
    core = lax.axis_index("sp") % 2
    widened_gain = gain[...]

    def normed(v):
        v = v.astype(jnp.float32)
        v = v * lax.rsqrt(jnp.mean(v * v, axis=-1, keepdims=True) + epsilon)
        return (v * widened_gain).astype(jnp.bfloat16)

    for b in range(BATCHES):
        mine = normed(tokens[core * BATCHES + b])
        theirs = normed(other[b])

        @pl.when(core == 1)
        def _():
            late[b] = mine
            early[b] = theirs

        @pl.when(core == 0)
        def _():
            late[b] = theirs
            early[b] = mine


def norm_rows(tokens, other, gain):
    shape = bf(BATCHES, PIECE, WIDTH)
    return pl.pallas_call(
        norm_body, out_shape=(shape, shape), in_specs=[VMEM] * 3, out_specs=(VMEM,) * 2,
        compiler_params=PARAMS, name="norm_rows",
    )(tokens, other, gain.reshape(1, WIDTH))


def row_copies(pieces, base, x_all, sems):
    t = lax.axis_index("tp")
    copies = []
    for d, piece in enumerate(pieces):
        at = pl.multiple_of(base + ((t + RING - d) % RING) * PIECE, PIECE)
        copies.append(pltpu.make_async_copy(piece, x_all.at[:, pl.ds(at, PIECE), :], sems.at[base // HALF, d]))
    return copies


def shard_copies(lines, first, count, w_all, sems, kind):
    core = lax.axis_index("sp") % 2
    copies = []
    for n, line in enumerate(lines):
        whose = core if n < RING else 1 - core
        for j in range(RING):
            at = pl.multiple_of(place_of(whose, j, n % RING, kind) * ROWS, ROWS)
            copies.append(
                pltpu.make_async_copy(
                    line.at[j, pl.ds(first, count)], w_all.at[pl.ds(first, count), pl.ds(at, ROWS), :],
                    sems.at[n * RING + j],
                )
            )
    return copies


def wide_pair_body(*refs):
    pieces, lines = refs[:4], refs[4:12]
    out, x_all, w_all, x_sems, w_sems = refs[12:]
    copies = row_copies(pieces, 0, x_all, x_sems) + shard_copies(lines, 0, 2, w_all, w_sems, 0)
    for c in copies:
        c.start()
    for c in copies:
        c.wait()
    for role in range(2):
        x = x_all[...].reshape(BATCHES * HALF, WIDTH)
        y = jnp.dot(x, w_all[role], preferred_element_type=jnp.float32)
        out[role] = y.astype(jnp.bfloat16).reshape(BATCHES, HALF, COLS)


def project_wide(pieces, lines):
    return pl.pallas_call(
        wide_pair_body, out_shape=bf(2, BATCHES, HALF, COLS), in_specs=[ANY] * 12, out_specs=VMEM,
        scratch_shapes=[
            pltpu.VMEM((BATCHES, HALF, WIDTH), jnp.bfloat16), pltpu.VMEM((2, WIDTH, COLS), jnp.bfloat16),
            pltpu.SemaphoreType.DMA((1, RING)), pltpu.SemaphoreType.DMA((32,)),
        ],
        compiler_params=PARAMS, name="project_wide",
    )(*pieces, *lines)


def rest_body(*refs):
    early, late, lines = refs[:4], refs[4:8], refs[8:16]
    near, near_tail, queries, x_all, w_all, x_sems, a_sems, b_sems, c_sems, d_sems = refs[16:]
    rows = row_copies(early, 0, x_all, x_sems) + row_copies(late, HALF, x_all, x_sems)
    groups = {
        0: rows + shard_copies(lines, 0, 1, w_all, a_sems, 0),
        1: shard_copies(lines, 1, 2, w_all, b_sems, 0),
        3: shard_copies(lines, 3, 2, w_all, c_sems, 0),
        5: shard_copies(lines, 5, 2, w_all, d_sems, 0),
    }
    following = {0: 1, 1: 3, 3: 5}
    for c in groups[0]:
        c.start()
    for m in range(NEAR + GROUPS):
        for c in groups.get(m, ()):
            c.wait()
        for c in groups.get(following.get(m), ()):
            c.start()
        x = x_all[...].reshape(BATCHES * SPAN, WIDTH)
        y = jnp.dot(x, w_all[m], preferred_element_type=jnp.float32)
        y = y.astype(jnp.bfloat16).reshape(BATCHES, SPAN, COLS)
        if m >= NEAR:
            queries[m - NEAR] = y
        else:
            near[m // 2, m % 2] = y
            if m < 2:
                near_tail[m % 2, :, : HALOS[0]] = y[:, SPAN - HALOS[0] :]
            else:
                near_tail[m % 2, :, HALOS[0] :] = y[:, SPAN - HALOS[1] :]


def project_rest(early, late, lines):
    return pl.pallas_call(
        rest_body,
        out_shape=(
            bf(2, 2, BATCHES, SPAN, COLS), bf(2, BATCHES, HALOS[0] + HALOS[1], COLS), bf(GROUPS, BATCHES, SPAN, COLS)
        ),
        in_specs=[ANY] * 16, out_specs=(VMEM,) * 3,
        scratch_shapes=[
            pltpu.VMEM((BATCHES, SPAN, WIDTH), jnp.bfloat16), pltpu.VMEM((NEAR + GROUPS, WIDTH, COLS), jnp.bfloat16),
            pltpu.SemaphoreType.DMA((2, RING)), pltpu.SemaphoreType.DMA((32,)), pltpu.SemaphoreType.DMA((32,)),
            pltpu.SemaphoreType.DMA((32,)), pltpu.SemaphoreType.DMA((32,)),
        ],
        compiler_params=PARAMS, name="project_rest",
    )(*early, *late, *lines)


def bias_of(group, block):
    halo, dilation = HALOS[group], DILATIONS[group]
    dims = (BLOCK, BLOCK + halo)
    q = lax.broadcasted_iota(jnp.int32, dims, 0)
    k = lax.broadcasted_iota(jnp.int32, dims, 1)
    lag = q + halo - k
    start = (lax.axis_index("sp") // 2) * SPAN + block * BLOCK - halo
    seen = (lag >= 0) & (lag <= STEPS * dilation) & ((lag & (dilation - 1)) == 0) & (k + start >= 0)
    return jnp.where(seen, 0.0, -1e30).astype(jnp.float32)


def attend(items):
    scores = [
        lax.dot_general(q, k, (((1,), (1,)), ((), ())), preferred_element_type=jnp.float32) for q, k, _, _ in items
    ]
    lifts = []
    for s, (_, _, _, bias) in zip(scores, items):
        s = s * (1.0 / math.sqrt(HEAD_WIDTH)) + bias
        peak = jnp.max(s, axis=-1, keepdims=True)
        lifted = jnp.exp(s - peak)
        lifts.append((lifted.astype(jnp.bfloat16), peak, jnp.sum(lifted, axis=-1, keepdims=True)))
    outs = [jnp.dot(p, v, preferred_element_type=jnp.float32) for (p, _, _), (_, _, v, _) in zip(lifts, items)]
    return [(o / total, peak + jnp.log(total)) for o, (_, peak, total) in zip(outs, lifts)]


def joined(o1, l1, o2, l2):
    top = jnp.maximum(l1, l2)
    a, c = jnp.exp(l1 - top), jnp.exp(l2 - top)
    total = a + c
    return (a * o1 + c * o2) / total, top + jnp.log(total)


PLACES = [
    (b, h, slice(h * HEAD_WIDTH, (h + 1) * HEAD_WIDTH)) for b in range(BATCHES) for h in range(COLS // HEAD_WIDTH)
]


def wide_body(q, early, late, back_early, back_late, far_late, out, logs, held, sems):
    copies = [
        pltpu.make_async_copy(part, held.at[:, :, pl.ds(n * HALF, HALF)], sems.at[n])
        for n, part in enumerate((far_late, back_early, back_late, early, late))
    ]
    for c in copies:
        c.start()
    for c in copies:
        c.wait()
    for i in range(SPAN // BLOCK):
        rows = slice(i * BLOCK, (i + 1) * BLOCK)
        keys = slice(i * BLOCK, (i + 1) * BLOCK + HALOS[2])
        bias = bias_of(2, i)
        found = attend([(q[b, rows, cols], held[0, b, keys, cols], held[1, b, keys, cols], bias) for b, _, cols in PLACES])
        for (b, _, cols), (o, l) in zip(PLACES, found):
            out[b, rows, cols] = o
            logs[b, rows, cols] = jnp.broadcast_to(l, (BLOCK, HEAD_WIDTH))


def attend_wide(q, early, late, back_early, back_late, far_late):
    shape = jax.ShapeDtypeStruct((BATCHES, SPAN, COLS), jnp.float32)
    return pl.pallas_call(
        wide_body, out_shape=(shape, shape),
        in_specs=[pl.BlockSpec((pl.squeezed, BATCHES, SPAN, COLS), lambda i: (2, 0, 0, 0))] + [ANY] * 5,
        out_specs=(VMEM,) * 2, grid=(1,),
        scratch_shapes=[
            pltpu.VMEM((2, BATCHES, HALOS[2] + SPAN, COLS), jnp.bfloat16), pltpu.SemaphoreType.DMA((5,)),
        ],
        compiler_params=PARAMS, name="attend_wide",
    )(q, early, late, back_early, back_late, far_late)


def near_body(q, near, tail, other, logs, c0, c1, c2, c3, kept, sent, k0, k1, mixed, weights, sems):
    copies = [
        pltpu.make_async_copy(tail.at[:, :, pl.ds(0, HALOS[0])], k0.at[:, :, pl.ds(0, HALOS[0])], sems.at[0]),
        pltpu.make_async_copy(tail.at[:, :, pl.ds(HALOS[0], HALOS[1])], k1.at[:, :, pl.ds(0, HALOS[1])], sems.at[1]),
        pltpu.make_async_copy(near.at[0], k0.at[:, :, pl.ds(HALOS[0], SPAN)], sems.at[2]),
        pltpu.make_async_copy(near.at[1], k1.at[:, :, pl.ds(HALOS[1], SPAN)], sems.at[3]),
    ]
    for c in copies:
        c.start()
    for c in copies:
        c.wait()
    core, t = lax.axis_index("sp") % 2, lax.axis_index("tp")
    for i in range(SPAN // BLOCK):
        rows = slice(i * BLOCK, (i + 1) * BLOCK)
        biases = [bias_of(g, i) for g in range(2)]
        for some in (PLACES[:3], PLACES[3:]):
            items = []
            for g, held in enumerate((k0, k1)):
                keys = slice(i * BLOCK, (i + 1) * BLOCK + HALOS[g])
                items += [
                    (q[g, b, rows, cols], held[0, b, keys, cols], held[1, b, keys, cols], biases[g]) for b, _, cols in some
                ]
            found = attend(items)
            for n, (b, h, cols) in enumerate(some):
                o, l = joined(*found[n], *found[n + 3])
                o, l = joined(o, l, other[b, rows, cols], logs[b, rows, cols])
                mixed[b, rows, cols] = o.astype(jnp.bfloat16)
                weights[i, 2 * b + h : 2 * b + h + 1, :] = jnp.transpose(l)[0:1]
    kept[...] = weights[core]
    sent[...] = weights[1 - core]
    for d, out in enumerate((c0, c1, c2, c3)):
        for far in range(2):
            whose = core if far == 0 else 1 - core
            at = pl.multiple_of(whose * HALF + ((t + d) % RING) * PIECE, PIECE)
            out[far] = mixed[:, pl.ds(at, PIECE), :]


def attend_near(q, near, tail, other, logs):
    piece = bf(2, BATCHES, PIECE, COLS)
    line = jax.ShapeDtypeStruct((2 * BATCHES, BLOCK), jnp.float32)
    return pl.pallas_call(
        near_body, out_shape=(piece,) * 4 + (line,) * 2, grid=(1,),
        in_specs=[pl.BlockSpec((2, BATCHES, SPAN, COLS), lambda i: (0, 0, 0, 0)), ANY, ANY, VMEM, VMEM],
        out_specs=(VMEM,) * 6,
        scratch_shapes=[
            pltpu.VMEM((2, BATCHES, HALOS[0] + SPAN, COLS), jnp.bfloat16),
            pltpu.VMEM((2, BATCHES, HALOS[1] + SPAN, COLS), jnp.bfloat16),
            pltpu.VMEM((BATCHES, SPAN, COLS), jnp.bfloat16),
            pltpu.VMEM((2, 2 * BATCHES, BLOCK), jnp.float32),
            pltpu.SemaphoreType.DMA((4,)),
        ],
        compiler_params=PARAMS, name="attend_near",
    )(q, near, tail, other, logs)


def lay_body(*refs):
    lines, out, sems = refs[:8], refs[8], refs[9]
    copies = shard_copies(lines, 0, RING, out, sems, 1)
    for c in copies:
        c.start()
    for c in copies:
        c.wait()


def lay_out(lines):
    return pl.pallas_call(
        lay_body, out_shape=bf(RING, WIDTH, COLS), in_specs=[ANY] * 8, out_specs=VMEM,
        scratch_shapes=[pltpu.SemaphoreType.DMA((32,))], compiler_params=PARAMS, name="lay_out",
    )(*lines)


def final_body(r0, r1, r2, r3, w, keep, send, w_all, sems):
    part = WIDTH // RING
    half = BATCHES * PIECE
    copies = [
        pltpu.make_async_copy(w.at[:, pl.ds(n * part, part)], w_all.at[n], sems.at[n]) for n in range(RING)
    ]
    for c in copies:
        c.start()
    rows = [r[...].reshape(2 * half, COLS) for r in (r0, r1, r2, r3)]
    for n in range(RING):
        cols = slice(n * part, (n + 1) * part)
        copies[n].wait()
        acc = None
        for d in range(RING):
            y = lax.dot_general(rows[d], w_all[n, d], (((1,), (1,)), ((), ())), preferred_element_type=jnp.float32)
            acc = y if acc is None else acc + y
        acc = acc.astype(jnp.bfloat16)
        keep[:, :, cols] = acc[:half].reshape(BATCHES, PIECE, part)
        send[:, :, cols] = acc[half:].reshape(BATCHES, PIECE, part)


def finish(received, w):
    shape = bf(BATCHES, PIECE, WIDTH)
    return pl.pallas_call(
        final_body, out_shape=(shape, shape), in_specs=[VMEM] * 4 + [ANY], out_specs=(VMEM,) * 2,
        scratch_shapes=[
            pltpu.VMEM((RING, RING, WIDTH // RING, COLS), jnp.bfloat16), pltpu.SemaphoreType.DMA((RING,)),
        ],
        compiler_params=PARAMS, name="finish",
    )(*received, w)


def joined_cores(mine, theirs):
    core = lax.axis_index("sp") % 2
    return jnp.where(core == 0, jnp.concatenate((mine, theirs), 0), jnp.concatenate((theirs, mine), 0))


def ring_of(a):
    came = {d: turned(a, d) for d in (1, 3, 2)}
    return [a, came[1], came[2], came[3]]


def spread(own, kind):
    near = {d: lax.ppermute(own, "sp", first_leg(d, kind)) for d in (1, 3, 2)}
    line = jnp.stack((own, near[1], near[2], near[3]))
    far = {d: lax.ppermute(line, "sp", second_leg(d, kind)) for d in (1, 3, 2)}
    lines = [line, far[1], far[2], far[3]]
    return lines + [swapped(a) for a in lines]


def layer(tokens, norm_gain, w_query, w_key, w_value, w_out):
    core = lax.axis_index("sp") % 2
    tokens = jnp.transpose(tokens, (1, 0, 2))
    send = lax.dynamic_slice_in_dim(tokens, (1 - core) * BATCHES, BATCHES, 0)
    other = swapped(send)
    wide_own, rest_own = pack(w_query, w_key, w_value)
    wide_lines = spread(wide_own, 0)
    late, early = norm_rows(tokens, other, norm_gain)
    late, early = ring_of(late), ring_of(early)
    rest_lines = spread(rest_own, 0)
    out_lines = spread(jnp.stack(ring_of(jnp.transpose(w_out))), 1)

    wide_late = project_wide(late, wide_lines)
    far_late = from_behind(wide_late, 2)
    back_late = from_behind(wide_late, 1)
    wide_early = project_wide(early, wide_lines)
    back_early = from_behind(wide_early, 1)
    near, near_tail, queries = project_rest(early, late, rest_lines)
    near_tail = from_behind(near_tail, 1)
    laid = lay_out(out_lines)
    wide_out, wide_logs = attend_wide(queries, wide_early, wide_late, back_early, back_late, far_late)
    *combined, kept, sent = attend_near(queries, near, near_tail, wide_out, wide_logs)

    received = [combined[0]] + [turned(combined[d], d) for d in (1, 2, 3)]
    mixed_mine, mixed_sent = finish(received, laid)
    mixed = joined_cores(mixed_mine, swapped(mixed_sent))

    log_weight = joined_cores(kept, swapped(sent)).reshape(2 * BATCHES, 2, BLOCK)
    return (jnp.transpose(mixed, (1, 0, 2)), jnp.transpose(log_weight, (2, 0, 1)))


def solution(mesh):
    in_specs = (
        P(("sp", "tp"), None, None),
        P(),
        P(None, "sp", "tp"),
        P(None, "sp", "tp"),
        P(None, "sp", "tp"),
        P("tp", "sp"),
    )
    out_specs = (P(("sp", "tp"), None, None), P("sp", None, "tp"))
    return jax.shard_map(layer, mesh=mesh, in_specs=in_specs, out_specs=out_specs, check_vma=False)
```

```python
import math

import jax
import jax.numpy as jnp
from jax import lax
from jax.experimental import pallas as pl
from jax.experimental.pallas import tpu as pltpu
from jax.sharding import PartitionSpec as P


GROUPS = 3
STEPS = 24
DILATIONS = (1, 4, 16)
HALOS = (32, 96, 384)
RING = 4
BATCHES = 3
PIECE = 32
SPAN = 256
HEAD_WIDTH = 128
COLS = 256
ROWS = 64
WIDTH = 2048
BLOCK = 128

epsilon = 1e-06


def chip(z, y, core):
    return (z % RING) * 8 + (y % RING) * 2 + core


def chips():
    return [(z, y, core) for z in range(RING) for y in range(RING) for core in range(2)]


def first_leg(shift, kind):
    def way(k):
        return k if kind == 0 else 0

    return [(chip(z, y, k), chip(z + shift * way(k), y + shift * (1 - way(k)), k)) for z, y, k in chips()]


def second_leg(shift, kind):
    def way(k):
        return k if kind == 0 else 0

    return [(chip(z, y, k), chip(z + shift * (1 - way(k)), y + shift * way(k), k)) for z, y, k in chips()]


SWAP = [(i, i ^ 1) for i in range(32)]


def swapped(a):
    return lax.ppermute(a, "sp", SWAP)


def turned(a, shift):
    return lax.ppermute(a, "tp", [(i, (i + shift) % RING) for i in range(RING)])


def from_behind(a, blocks):
    return lax.ppermute(a, "sp", [(i, i + 2 * blocks) for i in range(32 - 2 * blocks)])


def place_of(core, first, second, kind):
    s = lax.axis_index("sp")
    z, y = s // 8, (s // 2) % RING
    if kind == 0:
        up = jnp.where(core == 0, second, first)
        along = jnp.where(core == 0, first, second)
    else:
        up, along = second, first
    return ((z + RING - up) % RING) * 8 + ((y + RING - along) % RING) * 2 + core


ANY = pl.BlockSpec(memory_space=pl.ANY)
VMEM = pl.BlockSpec(memory_space=pltpu.VMEM)
PARAMS = pltpu.CompilerParams(vmem_limit_bytes=56 * 1024 * 1024)
HALF = SPAN // 2
NEAR = 4


def bf(*dims):
    return jax.ShapeDtypeStruct(dims, jnp.bfloat16)


def pack_body(w_query, w_key, w_value, wide, rest):
    wide[0] = w_key[2]
    wide[1] = w_value[2]
    for g in range(2):
        rest[2 * g] = w_key[g]
        rest[2 * g + 1] = w_value[g]
    rest[NEAR:] = w_query[...]


def pack(w_query, w_key, w_value):
    return pl.pallas_call(
        pack_body, out_shape=(bf(2, ROWS, COLS), bf(NEAR + GROUPS, ROWS, COLS)),
        in_specs=[VMEM] * 3, out_specs=(VMEM,) * 2, compiler_params=PARAMS, name="pack",
    )(w_query, w_key, w_value)


def norm_body(tokens, other, gain, late, early):
    core = lax.axis_index("sp") % 2
    widened_gain = gain[...]

    def normed(v):
        v = v.astype(jnp.float32)
        v = v * lax.rsqrt(jnp.mean(v * v, axis=-1, keepdims=True) + epsilon)
        return (v * widened_gain).astype(jnp.bfloat16)

    for b in range(BATCHES):
        mine = normed(tokens[core * BATCHES + b])
        theirs = normed(other[b])

        @pl.when(core == 1)
        def _():
            late[b] = mine
            early[b] = theirs

        @pl.when(core == 0)
        def _():
            late[b] = theirs
            early[b] = mine


def norm_rows(tokens, other, gain):
    shape = bf(BATCHES, PIECE, WIDTH)
    return pl.pallas_call(
        norm_body, out_shape=(shape, shape), in_specs=[VMEM] * 3, out_specs=(VMEM,) * 2,
        compiler_params=PARAMS, name="norm_rows",
    )(tokens, other, gain.reshape(1, WIDTH))


def row_copies(pieces, base, x_all, sems):
    t = lax.axis_index("tp")
    copies = []
    for d, piece in enumerate(pieces):
        at = pl.multiple_of(base + ((t + RING - d) % RING) * PIECE, PIECE)
        copies.append(pltpu.make_async_copy(piece, x_all.at[:, pl.ds(at, PIECE), :], sems.at[base // HALF, d]))
    return copies


def shard_copies(lines, first, count, w_all, sems, kind):
    core = lax.axis_index("sp") % 2
    copies = []
    for n, line in enumerate(lines):
        whose = core if n < RING else 1 - core
        for j in range(RING):
            at = pl.multiple_of(place_of(whose, j, n % RING, kind) * ROWS, ROWS)
            copies.append(
                pltpu.make_async_copy(
                    line.at[j, pl.ds(first, count)], w_all.at[pl.ds(first, count), pl.ds(at, ROWS), :],
                    sems.at[n * RING + j],
                )
            )
    return copies


def wide_pair_body(*refs):
    pieces, lines = refs[:4], refs[4:12]
    out, x_all, w_all, x_sems, w_sems = refs[12:]
    copies = row_copies(pieces, 0, x_all, x_sems) + shard_copies(lines, 0, 2, w_all, w_sems, 0)
    for c in copies:
        c.start()
    for c in copies:
        c.wait()
    for role in range(2):
        x = x_all[...].reshape(BATCHES * HALF, WIDTH)
        y = jnp.dot(x, w_all[role], preferred_element_type=jnp.float32)
        out[role] = y.astype(jnp.bfloat16).reshape(BATCHES, HALF, COLS)


def project_wide(pieces, lines):
    return pl.pallas_call(
        wide_pair_body, out_shape=bf(2, BATCHES, HALF, COLS), in_specs=[ANY] * 12, out_specs=VMEM,
        scratch_shapes=[
            pltpu.VMEM((BATCHES, HALF, WIDTH), jnp.bfloat16), pltpu.VMEM((2, WIDTH, COLS), jnp.bfloat16),
            pltpu.SemaphoreType.DMA((1, RING)), pltpu.SemaphoreType.DMA((32,)),
        ],
        compiler_params=PARAMS, name="project_wide",
    )(*pieces, *lines)


def matrix_copies(shards_of, first, count, w_all, sems):
    return [
        pltpu.make_async_copy(shards_of.at[:, first + m], w_all.at[m], sems.at[m]) for m in range(count)
    ]


def project(x_all, w_all, m):
    x = x_all[...].reshape(BATCHES * SPAN, WIDTH)
    y = jnp.dot(x, w_all[m].reshape(WIDTH, COLS), preferred_element_type=jnp.float32)
    return y.astype(jnp.bfloat16).reshape(BATCHES, SPAN, COLS)


def staged(early, late, rest, first, count, x_all, w_all, x_sems, w_sems, work):
    rows = row_copies(early, 0, x_all, x_sems) + row_copies(late, HALF, x_all, x_sems)
    weights = matrix_copies(rest, first, count, w_all, w_sems)
    for c in rows + weights[:1]:
        c.start()
    for c in rows:
        c.wait()
    for m in range(count):
        weights[m].wait()
        if m + 1 < count:
            weights[m + 1].start()
        work(m, project(x_all, w_all, m))


def near_pair_body(*refs):
    early, late, rest = refs[:4], refs[4:8], refs[8]
    near, near_tail, *scratch = refs[9:]

    def work(m, y):
        near[m // 2, m % 2] = y
        if m < 2:
            near_tail[m % 2, :, : HALOS[0]] = y[:, SPAN - HALOS[0] :]
        else:
            near_tail[m % 2, :, HALOS[0] :] = y[:, SPAN - HALOS[1] :]

    staged(early, late, rest, 0, NEAR, *scratch, work)


def query_body(*refs):
    early, late, rest = refs[:4], refs[4:8], refs[8]
    queries, *scratch = refs[9:]

    def work(m, y):
        queries[m] = y

    staged(early, late, rest, NEAR, GROUPS, *scratch, work)


def rest_scratch(count):
    return [
        pltpu.VMEM((BATCHES, SPAN, WIDTH), jnp.bfloat16), pltpu.VMEM((count, 32, ROWS, COLS), jnp.bfloat16),
        pltpu.SemaphoreType.DMA((2, RING)), pltpu.SemaphoreType.DMA((count,)),
    ]


def project_near(early, late, rest):
    return pl.pallas_call(
        near_pair_body,
        out_shape=(bf(2, 2, BATCHES, SPAN, COLS), bf(2, BATCHES, HALOS[0] + HALOS[1], COLS)),
        in_specs=[ANY] * 9, out_specs=(VMEM,) * 2, scratch_shapes=rest_scratch(NEAR),
        compiler_params=PARAMS, name="project_near",
    )(*early, *late, rest)


def project_queries(early, late, rest):
    return pl.pallas_call(
        query_body, out_shape=bf(GROUPS, BATCHES, SPAN, COLS),
        in_specs=[ANY] * 9, out_specs=VMEM, scratch_shapes=rest_scratch(GROUPS),
        compiler_params=PARAMS, name="project_queries",
    )(*early, *late, rest)


def bias_of(group, block):
    halo, dilation = HALOS[group], DILATIONS[group]
    dims = (BLOCK, BLOCK + halo)
    q = lax.broadcasted_iota(jnp.int32, dims, 0)
    k = lax.broadcasted_iota(jnp.int32, dims, 1)
    lag = q + halo - k
    start = (lax.axis_index("sp") // 2) * SPAN + block * BLOCK - halo
    seen = (lag >= 0) & (lag <= STEPS * dilation) & ((lag & (dilation - 1)) == 0) & (k + start >= 0)
    return jnp.where(seen, 0.0, -1e30).astype(jnp.float32)


def attend(items):
    scores = [
        lax.dot_general(q, k, (((1,), (1,)), ((), ())), preferred_element_type=jnp.float32) for q, k, _, _ in items
    ]
    lifts = []
    for s, (_, _, _, bias) in zip(scores, items):
        s = s * (1.0 / math.sqrt(HEAD_WIDTH)) + bias
        peak = jnp.max(s, axis=-1, keepdims=True)
        lifted = jnp.exp(s - peak)
        lifts.append((lifted.astype(jnp.bfloat16), peak, jnp.sum(lifted, axis=-1, keepdims=True)))
    outs = [jnp.dot(p, v, preferred_element_type=jnp.float32) for (p, _, _), (_, _, v, _) in zip(lifts, items)]
    return [(o / total, peak + jnp.log(total)) for o, (_, peak, total) in zip(outs, lifts)]


def joined(o1, l1, o2, l2):
    top = jnp.maximum(l1, l2)
    a, c = jnp.exp(l1 - top), jnp.exp(l2 - top)
    total = a + c
    return (a * o1 + c * o2) / total, top + jnp.log(total)


PLACES = [
    (b, h, slice(h * HEAD_WIDTH, (h + 1) * HEAD_WIDTH)) for b in range(BATCHES) for h in range(COLS // HEAD_WIDTH)
]


def wide_body(q, early, late, back_early, back_late, far_late, out, logs, held, sems):
    copies = [
        pltpu.make_async_copy(part, held.at[:, :, pl.ds(n * HALF, HALF)], sems.at[n])
        for n, part in enumerate((far_late, back_early, back_late, early, late))
    ]
    for c in copies:
        c.start()
    for c in copies:
        c.wait()
    for i in range(SPAN // BLOCK):
        rows = slice(i * BLOCK, (i + 1) * BLOCK)
        keys = slice(i * BLOCK, (i + 1) * BLOCK + HALOS[2])
        bias = bias_of(2, i)
        found = attend([(q[b, rows, cols], held[0, b, keys, cols], held[1, b, keys, cols], bias) for b, _, cols in PLACES])
        for (b, _, cols), (o, l) in zip(PLACES, found):
            out[b, rows, cols] = o
            logs[b, rows, cols] = jnp.broadcast_to(l, (BLOCK, HEAD_WIDTH))


def attend_wide(q, early, late, back_early, back_late, far_late):
    shape = jax.ShapeDtypeStruct((BATCHES, SPAN, COLS), jnp.float32)
    return pl.pallas_call(
        wide_body, out_shape=(shape, shape),
        in_specs=[pl.BlockSpec((pl.squeezed, BATCHES, SPAN, COLS), lambda i: (2, 0, 0, 0))] + [ANY] * 5,
        out_specs=(VMEM,) * 2, grid=(1,),
        scratch_shapes=[
            pltpu.VMEM((2, BATCHES, HALOS[2] + SPAN, COLS), jnp.bfloat16), pltpu.SemaphoreType.DMA((5,)),
        ],
        compiler_params=PARAMS, name="attend_wide",
    )(q, early, late, back_early, back_late, far_late)


def near_body(q, near, tail, other, logs, c0, c1, c2, c3, kept, sent, k0, k1, mixed, weights, sems):
    copies = [
        pltpu.make_async_copy(tail.at[:, :, pl.ds(0, HALOS[0])], k0.at[:, :, pl.ds(0, HALOS[0])], sems.at[0]),
        pltpu.make_async_copy(tail.at[:, :, pl.ds(HALOS[0], HALOS[1])], k1.at[:, :, pl.ds(0, HALOS[1])], sems.at[1]),
        pltpu.make_async_copy(near.at[0], k0.at[:, :, pl.ds(HALOS[0], SPAN)], sems.at[2]),
        pltpu.make_async_copy(near.at[1], k1.at[:, :, pl.ds(HALOS[1], SPAN)], sems.at[3]),
    ]
    for c in copies:
        c.start()
    for c in copies:
        c.wait()
    core, t = lax.axis_index("sp") % 2, lax.axis_index("tp")
    for i in range(SPAN // BLOCK):
        rows = slice(i * BLOCK, (i + 1) * BLOCK)
        biases = [bias_of(g, i) for g in range(2)]
        for some in (PLACES[:3], PLACES[3:]):
            items = []
            for g, held in enumerate((k0, k1)):
                keys = slice(i * BLOCK, (i + 1) * BLOCK + HALOS[g])
                items += [
                    (q[g, b, rows, cols], held[0, b, keys, cols], held[1, b, keys, cols], biases[g]) for b, _, cols in some
                ]
            found = attend(items)
            for n, (b, h, cols) in enumerate(some):
                o, l = joined(*found[n], *found[n + 3])
                o, l = joined(o, l, other[b, rows, cols], logs[b, rows, cols])
                mixed[b, rows, cols] = o.astype(jnp.bfloat16)
                weights[i, 2 * b + h : 2 * b + h + 1, :] = jnp.transpose(l)[0:1]
    kept[...] = weights[core]
    sent[...] = weights[1 - core]
    for d, out in enumerate((c0, c1, c2, c3)):
        for far in range(2):
            whose = core if far == 0 else 1 - core
            at = pl.multiple_of(whose * HALF + ((t + d) % RING) * PIECE, PIECE)
            out[far] = mixed[:, pl.ds(at, PIECE), :]


def attend_near(q, near, tail, other, logs):
    piece = bf(2, BATCHES, PIECE, COLS)
    line = jax.ShapeDtypeStruct((2 * BATCHES, BLOCK), jnp.float32)
    return pl.pallas_call(
        near_body, out_shape=(piece,) * 4 + (line,) * 2, grid=(1,),
        in_specs=[pl.BlockSpec((2, BATCHES, SPAN, COLS), lambda i: (0, 0, 0, 0)), ANY, ANY, VMEM, VMEM],
        out_specs=(VMEM,) * 6,
        scratch_shapes=[
            pltpu.VMEM((2, BATCHES, HALOS[0] + SPAN, COLS), jnp.bfloat16),
            pltpu.VMEM((2, BATCHES, HALOS[1] + SPAN, COLS), jnp.bfloat16),
            pltpu.VMEM((BATCHES, SPAN, COLS), jnp.bfloat16),
            pltpu.VMEM((2, 2 * BATCHES, BLOCK), jnp.float32),
            pltpu.SemaphoreType.DMA((4,)),
        ],
        compiler_params=PARAMS, name="attend_near",
    )(q, near, tail, other, logs)


def final_body(r0, r1, r2, r3, w, keep, send, w_all, sems):
    t = lax.axis_index("tp")
    part = WIDTH // RING
    half = BATCHES * PIECE
    count = part // ROWS
    copies = [
        [
            pltpu.make_async_copy(
                w.at[pl.ds(n * count, count), (t + RING - d) % RING], w_all.at[n, d], sems.at[n, d]
            )
            for d in range(RING)
        ]
        for n in range(RING)
    ]
    for group in copies:
        for c in group:
            c.start()
    rows = [r[...].reshape(2 * half, COLS) for r in (r0, r1, r2, r3)]
    for n in range(RING):
        cols = slice(n * part, (n + 1) * part)
        for c in copies[n]:
            c.wait()
        acc = None
        for d in range(RING):
            block = w_all[n, d].reshape(part, COLS)
            y = lax.dot_general(rows[d], block, (((1,), (1,)), ((), ())), preferred_element_type=jnp.float32)
            acc = y if acc is None else acc + y
        acc = acc.astype(jnp.bfloat16)
        keep[:, :, cols] = acc[:half].reshape(BATCHES, PIECE, part)
        send[:, :, cols] = acc[half:].reshape(BATCHES, PIECE, part)


def finish(received, w):
    shape = bf(BATCHES, PIECE, WIDTH)
    return pl.pallas_call(
        final_body, out_shape=(shape, shape), in_specs=[VMEM] * 4 + [ANY], out_specs=(VMEM,) * 2,
        scratch_shapes=[
            pltpu.VMEM((RING, RING, WIDTH // RING // ROWS, ROWS, COLS), jnp.bfloat16),
            pltpu.SemaphoreType.DMA((RING, RING)),
        ],
        compiler_params=PARAMS, name="finish",
    )(*received, w)


def joined_cores(mine, theirs):
    core = lax.axis_index("sp") % 2
    return jnp.where(core == 0, jnp.concatenate((mine, theirs), 0), jnp.concatenate((theirs, mine), 0))


def merge_body(mine, theirs, out, sems):
    core = lax.axis_index("sp") % 2
    copies = [
        pltpu.make_async_copy(mine, out.at[pl.ds(core * BATCHES, BATCHES)], sems.at[0]),
        pltpu.make_async_copy(theirs, out.at[pl.ds((1 - core) * BATCHES, BATCHES)], sems.at[1]),
    ]
    for c in copies:
        c.start()
    for c in copies:
        c.wait()


def merged(mine, theirs):
    return pl.pallas_call(
        merge_body, out_shape=bf(2 * BATCHES, PIECE, WIDTH), in_specs=[ANY] * 2, out_specs=ANY,
        scratch_shapes=[pltpu.SemaphoreType.DMA((2,))], compiler_params=PARAMS, name="merge",
    )(mine, theirs)


def ring_of(a):
    came = {d: turned(a, d) for d in (1, 3, 2)}
    return [a, came[1], came[2], came[3]]


def spread(own, kind):
    near = {d: lax.ppermute(own, "sp", first_leg(d, kind)) for d in (1, 3, 2)}
    line = jnp.stack((own, near[1], near[2], near[3]))
    far = {d: lax.ppermute(line, "sp", second_leg(d, kind)) for d in (1, 3, 2)}
    lines = [line, far[1], far[2], far[3]]
    return lines + [swapped(a) for a in lines]


def layer(tokens, norm_gain, w_query, w_key, w_value, w_out):
    wide_own, rest_own = pack(w_query, w_key, w_value)
    rest = lax.all_gather(rest_own, "sp")
    outs = lax.all_gather(jnp.transpose(w_out), ("sp", "tp"))
    outs = outs.reshape(32, RING, ROWS, COLS)

    core = lax.axis_index("sp") % 2
    tokens = jnp.transpose(tokens, (1, 0, 2))
    send = lax.dynamic_slice_in_dim(tokens, (1 - core) * BATCHES, BATCHES, 0)
    other = swapped(send)
    wide_lines = spread(wide_own, 0)
    late, early = norm_rows(tokens, other, norm_gain)
    late, early = ring_of(late), ring_of(early)

    wide_late = project_wide(late, wide_lines)
    far_late = from_behind(wide_late, 2)
    back_late = from_behind(wide_late, 1)
    wide_early = project_wide(early, wide_lines)
    back_early = from_behind(wide_early, 1)
    near, near_tail = project_near(early, late, rest)
    near_tail = from_behind(near_tail, 1)
    queries = project_queries(early, late, rest)
    wide_out, wide_logs = attend_wide(queries, wide_early, wide_late, back_early, back_late, far_late)
    *combined, kept, sent = attend_near(queries, near, near_tail, wide_out, wide_logs)

    received = [combined[0]] + [turned(combined[d], d) for d in (1, 2, 3)]
    mixed_mine, mixed_sent = finish(received, outs)
    mixed = merged(mixed_mine, swapped(mixed_sent))

    log_weight = joined_cores(kept, swapped(sent)).reshape(2 * BATCHES, 2, BLOCK)
    return (jnp.transpose(mixed, (1, 0, 2)), jnp.transpose(log_weight, (2, 0, 1)))


def solution(mesh):
    in_specs = (
        P(("sp", "tp"), None, None),
        P(),
        P(None, "sp", "tp"),
        P(None, "sp", "tp"),
        P(None, "sp", "tp"),
        P("tp", "sp"),
    )
    out_specs = (P(("sp", "tp"), None, None), P("sp", None, "tp"))
    return jax.shard_map(layer, mesh=mesh, in_specs=in_specs, out_specs=out_specs, check_vma=False)
```

```python
import math

import jax
import jax.numpy as jnp
from jax import lax
from jax.experimental import pallas as pl
from jax.experimental.pallas import tpu as pltpu
from jax.sharding import PartitionSpec as P


GROUPS = 3
STEPS = 24
DILATIONS = (1, 4, 16)
HALOS = (32, 96, 384)
RING = 4
BATCHES = 3
PIECE = 32
SPAN = 256
HEAD_WIDTH = 128
COLS = 256
ROWS = 64
WIDTH = 2048
BLOCK = 128

epsilon = 1e-06


def chip(z, y, core):
    return (z % RING) * 8 + (y % RING) * 2 + core


def chips():
    return [(z, y, core) for z in range(RING) for y in range(RING) for core in range(2)]


def first_leg(shift, kind):
    def way(k):
        return k if kind == 0 else 0

    return [(chip(z, y, k), chip(z + shift * way(k), y + shift * (1 - way(k)), k)) for z, y, k in chips()]


def second_leg(shift, kind):
    def way(k):
        return k if kind == 0 else 0

    return [(chip(z, y, k), chip(z + shift * (1 - way(k)), y + shift * way(k), k)) for z, y, k in chips()]


SWAP = [(i, i ^ 1) for i in range(32)]


def swapped(a):
    return lax.ppermute(a, "sp", SWAP)


def turned(a, shift):
    return lax.ppermute(a, "tp", [(i, (i + shift) % RING) for i in range(RING)])


def from_behind(a, blocks):
    return lax.ppermute(a, "sp", [(i, i + 2 * blocks) for i in range(32 - 2 * blocks)])


def place_of(core, first, second, kind):
    s = lax.axis_index("sp")
    z, y = s // 8, (s // 2) % RING
    if kind == 0:
        up = jnp.where(core == 0, second, first)
        along = jnp.where(core == 0, first, second)
    else:
        up, along = second, first
    return ((z + RING - up) % RING) * 8 + ((y + RING - along) % RING) * 2 + core


ANY = pl.BlockSpec(memory_space=pl.ANY)
VMEM = pl.BlockSpec(memory_space=pltpu.VMEM)
PARAMS = pltpu.CompilerParams(vmem_limit_bytes=56 * 1024 * 1024)
HALF = SPAN // 2
NEAR = 4
LAST = NEAR + GROUPS


def bf(*dims):
    return jax.ShapeDtypeStruct(dims, jnp.bfloat16)


def pack_body(w_query, w_key, w_value, w_out, wide, rest):
    wide[0] = w_key[2]
    wide[1] = w_value[2]
    for g in range(2):
        rest[2 * g] = w_key[g]
        rest[2 * g + 1] = w_value[g]
    rest[NEAR:LAST] = w_query[...]
    rest[LAST] = w_out[...]


def pack(w_query, w_key, w_value, w_out):
    return pl.pallas_call(
        pack_body, out_shape=(bf(2, ROWS, COLS), bf(LAST + 1, ROWS, COLS)),
        in_specs=[VMEM] * 4, out_specs=(VMEM,) * 2, compiler_params=PARAMS, name="pack",
    )(w_query, w_key, w_value, jnp.transpose(w_out))


def norm_body(tokens, other, gain, late, early):
    core = lax.axis_index("sp") % 2
    widened_gain = gain[...]

    def normed(v):
        v = v.astype(jnp.float32)
        v = v * lax.rsqrt(jnp.mean(v * v, axis=-1, keepdims=True) + epsilon)
        return (v * widened_gain).astype(jnp.bfloat16)

    for b in range(BATCHES):
        mine = normed(tokens[core * BATCHES + b])
        theirs = normed(other[b])

        @pl.when(core == 1)
        def _():
            late[b] = mine
            early[b] = theirs

        @pl.when(core == 0)
        def _():
            late[b] = theirs
            early[b] = mine


def norm_rows(tokens, other, gain):
    shape = bf(BATCHES, PIECE, WIDTH)
    return pl.pallas_call(
        norm_body, out_shape=(shape, shape), in_specs=[VMEM] * 3, out_specs=(VMEM,) * 2,
        compiler_params=PARAMS, name="norm_rows",
    )(tokens, other, gain.reshape(1, WIDTH))


def row_copies(pieces, base, x_all, sems):
    t = lax.axis_index("tp")
    copies = []
    for d, piece in enumerate(pieces):
        at = pl.multiple_of(base + ((t + RING - d) % RING) * PIECE, PIECE)
        copies.append(pltpu.make_async_copy(piece, x_all.at[:, pl.ds(at, PIECE), :], sems.at[base // HALF, d]))
    return copies


def shard_copies(lines, first, count, w_all, sems, kind):
    core = lax.axis_index("sp") % 2
    copies = []
    for n, line in enumerate(lines):
        whose = core if n < RING else 1 - core
        for j in range(RING):
            at = pl.multiple_of(place_of(whose, j, n % RING, kind) * ROWS, ROWS)
            copies.append(
                pltpu.make_async_copy(
                    line.at[j, pl.ds(first, count)], w_all.at[pl.ds(first, count), pl.ds(at, ROWS), :],
                    sems.at[n * RING + j],
                )
            )
    return copies


def wide_pair_body(*refs):
    pieces, lines = refs[:4], refs[4:12]
    out, x_all, w_all, x_sems, w_sems = refs[12:]
    copies = row_copies(pieces, 0, x_all, x_sems) + shard_copies(lines, 0, 2, w_all, w_sems, 0)
    for c in copies:
        c.start()
    for c in copies:
        c.wait()
    for role in range(2):
        x = x_all[...].reshape(BATCHES * HALF, WIDTH)
        y = jnp.dot(x, w_all[role], preferred_element_type=jnp.float32)
        out[role] = y.astype(jnp.bfloat16).reshape(BATCHES, HALF, COLS)


def project_wide(pieces, lines):
    return pl.pallas_call(
        wide_pair_body, out_shape=bf(2, BATCHES, HALF, COLS), in_specs=[ANY] * 12, out_specs=VMEM,
        scratch_shapes=[
            pltpu.VMEM((BATCHES, HALF, WIDTH), jnp.bfloat16), pltpu.VMEM((2, WIDTH, COLS), jnp.bfloat16),
            pltpu.SemaphoreType.DMA((1, RING)), pltpu.SemaphoreType.DMA((32,)),
        ],
        compiler_params=PARAMS, name="project_wide",
    )(*pieces, *lines)


def matrix_copies(shards_of, first, count, w_all, sems):
    return [
        pltpu.make_async_copy(shards_of.at[:, first + m], w_all.at[m], sems.at[m]) for m in range(count)
    ]


def project(x_all, w_all, m):
    x = x_all[...].reshape(BATCHES * SPAN, WIDTH)
    y = jnp.dot(x, w_all[m].reshape(WIDTH, COLS), preferred_element_type=jnp.float32)
    return y.astype(jnp.bfloat16).reshape(BATCHES, SPAN, COLS)


def staged(early, late, rest, first, count, x_all, w_all, x_sems, w_sems, work):
    rows = row_copies(early, 0, x_all, x_sems) + row_copies(late, HALF, x_all, x_sems)
    weights = matrix_copies(rest, first, count, w_all, w_sems)
    for c in rows + weights[:2]:
        c.start()
    for c in rows:
        c.wait()
    for m in range(count):
        weights[m].wait()
        if m + 2 < count:
            weights[m + 2].start()
        work(m, project(x_all, w_all, m))


def near_pair_body(*refs):
    early, late, rest = refs[:4], refs[4:8], refs[8]
    near, near_tail, *scratch = refs[9:]

    def work(m, y):
        near[m // 2, m % 2] = y
        if m < 2:
            near_tail[m % 2, :, : HALOS[0]] = y[:, SPAN - HALOS[0] :]
        else:
            near_tail[m % 2, :, HALOS[0] :] = y[:, SPAN - HALOS[1] :]

    staged(early, late, rest, 0, NEAR, *scratch, work)


def query_body(*refs):
    early, late, rest = refs[:4], refs[4:8], refs[8]
    queries, *scratch = refs[9:]

    def work(m, y):
        queries[m] = y

    staged(early, late, rest, NEAR, GROUPS, *scratch, work)


def rest_scratch(count):
    return [
        pltpu.VMEM((BATCHES, SPAN, WIDTH), jnp.bfloat16), pltpu.VMEM((count, 32, ROWS, COLS), jnp.bfloat16),
        pltpu.SemaphoreType.DMA((2, RING)), pltpu.SemaphoreType.DMA((count,)),
    ]


def project_near(early, late, rest):
    return pl.pallas_call(
        near_pair_body,
        out_shape=(bf(2, 2, BATCHES, SPAN, COLS), bf(2, BATCHES, HALOS[0] + HALOS[1], COLS)),
        in_specs=[ANY] * 9, out_specs=(VMEM,) * 2, scratch_shapes=rest_scratch(NEAR),
        compiler_params=PARAMS, name="project_near",
    )(*early, *late, rest)


def project_queries(early, late, rest):
    return pl.pallas_call(
        query_body, out_shape=bf(GROUPS, BATCHES, SPAN, COLS),
        in_specs=[ANY] * 9, out_specs=VMEM, scratch_shapes=rest_scratch(GROUPS),
        compiler_params=PARAMS, name="project_queries",
    )(*early, *late, rest)


def bias_of(group, block):
    halo, dilation = HALOS[group], DILATIONS[group]
    dims = (BLOCK, BLOCK + halo)
    q = lax.broadcasted_iota(jnp.int32, dims, 0)
    k = lax.broadcasted_iota(jnp.int32, dims, 1)
    lag = q + halo - k
    start = (lax.axis_index("sp") // 2) * SPAN + block * BLOCK - halo
    seen = (lag >= 0) & (lag <= STEPS * dilation) & ((lag & (dilation - 1)) == 0) & (k + start >= 0)
    return jnp.where(seen, 0.0, -1e30).astype(jnp.float32)


def attend(items):
    scores = [
        lax.dot_general(q, k, (((1,), (1,)), ((), ())), preferred_element_type=jnp.float32) for q, k, _, _ in items
    ]
    lifts = []
    for s, (_, _, _, bias) in zip(scores, items):
        s = s * (1.0 / math.sqrt(HEAD_WIDTH)) + bias
        peak = jnp.max(s, axis=-1, keepdims=True)
        lifted = jnp.exp(s - peak)
        lifts.append((lifted.astype(jnp.bfloat16), peak, jnp.sum(lifted, axis=-1, keepdims=True)))
    outs = [jnp.dot(p, v, preferred_element_type=jnp.float32) for (p, _, _), (_, _, v, _) in zip(lifts, items)]
    return [(o / total, peak + jnp.log(total)) for o, (_, peak, total) in zip(outs, lifts)]


def joined(o1, l1, o2, l2):
    top = jnp.maximum(l1, l2)
    a, c = jnp.exp(l1 - top), jnp.exp(l2 - top)
    total = a + c
    return (a * o1 + c * o2) / total, top + jnp.log(total)


PLACES = [
    (b, h, slice(h * HEAD_WIDTH, (h + 1) * HEAD_WIDTH)) for b in range(BATCHES) for h in range(COLS // HEAD_WIDTH)
]


def wide_body(q, early, late, back_early, back_late, far_late, out, logs, held, sems):
    copies = [
        pltpu.make_async_copy(part, held.at[:, :, pl.ds(n * HALF, HALF)], sems.at[n])
        for n, part in enumerate((far_late, back_early, back_late, early, late))
    ]
    for c in copies:
        c.start()
    for c in copies:
        c.wait()
    for i in range(SPAN // BLOCK):
        rows = slice(i * BLOCK, (i + 1) * BLOCK)
        keys = slice(i * BLOCK, (i + 1) * BLOCK + HALOS[2])
        bias = bias_of(2, i)
        found = attend([(q[b, rows, cols], held[0, b, keys, cols], held[1, b, keys, cols], bias) for b, _, cols in PLACES])
        for (b, _, cols), (o, l) in zip(PLACES, found):
            out[b, rows, cols] = o
            logs[b, rows, cols] = jnp.broadcast_to(l, (BLOCK, HEAD_WIDTH))


def attend_wide(q, early, late, back_early, back_late, far_late):
    shape = jax.ShapeDtypeStruct((BATCHES, SPAN, COLS), jnp.float32)
    return pl.pallas_call(
        wide_body, out_shape=(shape, shape),
        in_specs=[pl.BlockSpec((pl.squeezed, BATCHES, SPAN, COLS), lambda i: (2, 0, 0, 0))] + [ANY] * 5,
        out_specs=(VMEM,) * 2, grid=(1,),
        scratch_shapes=[
            pltpu.VMEM((2, BATCHES, HALOS[2] + SPAN, COLS), jnp.bfloat16), pltpu.SemaphoreType.DMA((5,)),
        ],
        compiler_params=PARAMS, name="attend_wide",
    )(q, early, late, back_early, back_late, far_late)


def near_body(q, near, tail, other, logs, c0, c1, c2, c3, kept, sent, k0, k1, mixed, weights, sems):
    copies = [
        pltpu.make_async_copy(tail.at[:, :, pl.ds(0, HALOS[0])], k0.at[:, :, pl.ds(0, HALOS[0])], sems.at[0]),
        pltpu.make_async_copy(tail.at[:, :, pl.ds(HALOS[0], HALOS[1])], k1.at[:, :, pl.ds(0, HALOS[1])], sems.at[1]),
        pltpu.make_async_copy(near.at[0], k0.at[:, :, pl.ds(HALOS[0], SPAN)], sems.at[2]),
        pltpu.make_async_copy(near.at[1], k1.at[:, :, pl.ds(HALOS[1], SPAN)], sems.at[3]),
    ]
    for c in copies:
        c.start()
    for c in copies:
        c.wait()
    core, t = lax.axis_index("sp") % 2, lax.axis_index("tp")
    for i in range(SPAN // BLOCK):
        rows = slice(i * BLOCK, (i + 1) * BLOCK)
        biases = [bias_of(g, i) for g in range(2)]
        for some in (PLACES[:3], PLACES[3:]):
            items = []
            for g, held in enumerate((k0, k1)):
                keys = slice(i * BLOCK, (i + 1) * BLOCK + HALOS[g])
                items += [
                    (q[g, b, rows, cols], held[0, b, keys, cols], held[1, b, keys, cols], biases[g]) for b, _, cols in some
                ]
            found = attend(items)
            for n, (b, h, cols) in enumerate(some):
                o, l = joined(*found[n], *found[n + 3])
                o, l = joined(o, l, other[b, rows, cols], logs[b, rows, cols])
                mixed[b, rows, cols] = o.astype(jnp.bfloat16)
                weights[i, 2 * b + h : 2 * b + h + 1, :] = jnp.transpose(l)[0:1]
    kept[...] = weights[core]
    sent[...] = weights[1 - core]
    for d, out in enumerate((c0, c1, c2, c3)):
        for far in range(2):
            whose = core if far == 0 else 1 - core
            at = pl.multiple_of(whose * HALF + ((t + d) % RING) * PIECE, PIECE)
            out[far] = mixed[:, pl.ds(at, PIECE), :]


def attend_near(q, near, tail, other, logs):
    piece = bf(2, BATCHES, PIECE, COLS)
    line = jax.ShapeDtypeStruct((2 * BATCHES, BLOCK), jnp.float32)
    return pl.pallas_call(
        near_body, out_shape=(piece,) * 4 + (line,) * 2, grid=(1,),
        in_specs=[pl.BlockSpec((2, BATCHES, SPAN, COLS), lambda i: (0, 0, 0, 0)), ANY, ANY, VMEM, VMEM],
        out_specs=(VMEM,) * 6,
        scratch_shapes=[
            pltpu.VMEM((2, BATCHES, HALOS[0] + SPAN, COLS), jnp.bfloat16),
            pltpu.VMEM((2, BATCHES, HALOS[1] + SPAN, COLS), jnp.bfloat16),
            pltpu.VMEM((BATCHES, SPAN, COLS), jnp.bfloat16),
            pltpu.VMEM((2, 2 * BATCHES, BLOCK), jnp.float32),
            pltpu.SemaphoreType.DMA((4,)),
        ],
        compiler_params=PARAMS, name="attend_near",
    )(q, near, tail, other, logs)


def final_body(r0, r1, r2, r3, rest, p1, p2, p3, q1, q2, q3, keep, send, w_all, sems):
    core = lax.axis_index("sp") % 2
    part = WIDTH // RING
    half = BATCHES * PIECE
    count = part // ROWS

    def copy(source, n, d):
        return pltpu.make_async_copy(source, w_all.at[n, d], sems.at[n, d])

    for m in range(2):
        for n in (m, m + 2):
            copy(rest.at[pl.ds(n * count, count), LAST], n, 0).start()
        for d, (p, q) in enumerate(((p1, q1), (p2, q2), (p3, q3)), 1):
            copy(p.at[pl.ds(m * count, count)], 2 * core + m, d).start()
            copy(q.at[pl.ds(m * count, count)], 2 * (1 - core) + m, d).start()
    rows = [r[...].reshape(2 * half, COLS) for r in (r0, r1, r2, r3)]
    for n in (0, 2, 1, 3):
        cols = slice(n * part, (n + 1) * part)
        for d in range(RING):
            copy(p1.at[pl.ds(0, count)], n, d).wait()
        acc = None
        for d in range(RING):
            block = w_all[n, d].reshape(part, COLS)
            y = lax.dot_general(rows[d], block, (((1,), (1,)), ((), ())), preferred_element_type=jnp.float32)
            acc = y if acc is None else acc + y
        acc = acc.astype(jnp.bfloat16)
        keep[:, :, cols] = acc[:half].reshape(BATCHES, PIECE, part)
        send[:, :, cols] = acc[half:].reshape(BATCHES, PIECE, part)


def finish(received, rest, pieces, crossed):
    shape = bf(BATCHES, PIECE, WIDTH)
    return pl.pallas_call(
        final_body, out_shape=(shape, shape), in_specs=[VMEM] * 4 + [ANY] * 7, out_specs=(VMEM,) * 2,
        scratch_shapes=[
            pltpu.VMEM((RING, RING, WIDTH // RING // ROWS, ROWS, COLS), jnp.bfloat16),
            pltpu.SemaphoreType.DMA((RING, RING)),
        ],
        compiler_params=PARAMS, name="finish",
    )(*received, rest, *pieces, *crossed)


def joined_cores(mine, theirs):
    core = lax.axis_index("sp") % 2
    return jnp.where(core == 0, jnp.concatenate((mine, theirs), 0), jnp.concatenate((theirs, mine), 0))


def merge_body(mine, theirs, out):
    core = lax.axis_index("sp") % 2
    out[pl.ds(core * BATCHES, BATCHES)] = mine[...]
    out[pl.ds((1 - core) * BATCHES, BATCHES)] = theirs[...]


def merged(mine, theirs):
    return pl.pallas_call(
        merge_body, out_shape=bf(2 * BATCHES, PIECE, WIDTH), in_specs=[VMEM] * 2, out_specs=VMEM,
        compiler_params=PARAMS, name="merge",
    )(mine, theirs)


def ring_of(a):
    came = {d: turned(a, d) for d in (1, 3, 2)}
    return [a, came[1], came[2], came[3]]


def spread(own, kind):
    near = {d: lax.ppermute(own, "sp", first_leg(d, kind)) for d in (1, 3, 2)}
    line = jnp.stack((own, near[1], near[2], near[3]))
    far = {d: lax.ppermute(line, "sp", second_leg(d, kind)) for d in (1, 3, 2)}
    lines = [line, far[1], far[2], far[3]]
    return lines + [swapped(a) for a in lines]


def layer(tokens, norm_gain, w_query, w_key, w_value, w_out):
    wide_own, rest_own = pack(w_query, w_key, w_value, w_out)
    rest = lax.all_gather(rest_own, "sp")

    core = lax.axis_index("sp") % 2
    tokens = jnp.transpose(tokens, (1, 0, 2))
    send = lax.dynamic_slice_in_dim(tokens, (1 - core) * BATCHES, BATCHES, 0)
    other = swapped(send)
    wide_lines = spread(wide_own, 0)
    late, early = norm_rows(tokens, other, norm_gain)
    late, early = ring_of(late), ring_of(early)

    wide_late = project_wide(late, wide_lines)
    far_late = from_behind(wide_late, 2)
    back_late = from_behind(wide_late, 1)
    wide_early = project_wide(early, wide_lines)
    back_early = from_behind(wide_early, 1)
    near, near_tail = project_near(early, late, rest)
    near_tail = from_behind(near_tail, 1)
    outs = lax.dynamic_slice(rest, (16 * core, LAST, 0, 0), (16, 1, ROWS, COLS))[:, 0]
    outs = ring_of(outs)[1:]
    queries = project_queries(early, late, rest)
    wide_out, wide_logs = attend_wide(queries, wide_early, wide_late, back_early, back_late, far_late)
    *combined, kept, sent = attend_near(queries, near, near_tail, wide_out, wide_logs)

    received = [combined[0]] + [turned(combined[d], d) for d in (1, 2, 3)]
    mixed_mine, mixed_sent = finish(received, rest, outs, [swapped(a) for a in outs])
    mixed = merged(mixed_mine, swapped(mixed_sent))

    log_weight = joined_cores(kept, swapped(sent)).reshape(2 * BATCHES, 2, BLOCK)
    return (jnp.transpose(mixed, (1, 0, 2)), jnp.transpose(log_weight, (2, 0, 1)))


def solution(mesh):
    in_specs = (
        P(("sp", "tp"), None, None),
        P(),
        P(None, "sp", "tp"),
        P(None, "sp", "tp"),
        P(None, "sp", "tp"),
        P("tp", "sp"),
    )
    out_specs = (P(("sp", "tp"), None, None), P("sp", None, "tp"))
    return jax.shard_map(layer, mesh=mesh, in_specs=in_specs, out_specs=out_specs, check_vma=False)
```

```python
import math

import jax
import jax.numpy as jnp
from jax import lax
from jax.experimental import pallas as pl
from jax.experimental.pallas import tpu as pltpu
from jax.sharding import PartitionSpec as P


GROUPS = 3
STEPS = 24
DILATIONS = (1, 4, 16)
HALOS = (32, 96, 384)
RING = 4
BATCHES = 3
PIECE = 32
SPAN = 256
HEAD_WIDTH = 128
COLS = 256
ROWS = 64
WIDTH = 2048
BLOCK = 128

epsilon = 1e-06


def chip(z, y, core):
    return (z % RING) * 8 + (y % RING) * 2 + core


def chips():
    return [(z, y, core) for z in range(RING) for y in range(RING) for core in range(2)]


def first_leg(shift, kind):
    def way(k):
        return k if kind == 0 else 0

    return [(chip(z, y, k), chip(z + shift * way(k), y + shift * (1 - way(k)), k)) for z, y, k in chips()]


def second_leg(shift, kind):
    def way(k):
        return k if kind == 0 else 0

    return [(chip(z, y, k), chip(z + shift * (1 - way(k)), y + shift * way(k), k)) for z, y, k in chips()]


SWAP = [(i, i ^ 1) for i in range(32)]


def swapped(a):
    return lax.ppermute(a, "sp", SWAP)


def turned(a, shift):
    return lax.ppermute(a, "tp", [(i, (i + shift) % RING) for i in range(RING)])


def from_behind(a, blocks):
    return lax.ppermute(a, "sp", [(i, i + 2 * blocks) for i in range(32 - 2 * blocks)])


def place_of(core, first, second, kind):
    s = lax.axis_index("sp")
    z, y = s // 8, (s // 2) % RING
    if kind == 0:
        up = jnp.where(core == 0, second, first)
        along = jnp.where(core == 0, first, second)
    else:
        up, along = second, first
    return ((z + RING - up) % RING) * 8 + ((y + RING - along) % RING) * 2 + core


ANY = pl.BlockSpec(memory_space=pl.ANY)
VMEM = pl.BlockSpec(memory_space=pltpu.VMEM)
PARAMS = pltpu.CompilerParams(vmem_limit_bytes=56 * 1024 * 1024)
HALF = SPAN // 2
NEAR = 4
LAST = NEAR + GROUPS


def bf(*dims):
    return jax.ShapeDtypeStruct(dims, jnp.bfloat16)


def pack_body(w_query, w_key, w_value, w_out, wide, rest):
    wide[0] = w_key[2]
    wide[1] = w_value[2]
    for g in range(2):
        rest[2 * g] = w_key[g]
        rest[2 * g + 1] = w_value[g]
    rest[NEAR:LAST] = w_query[...]
    rest[LAST] = w_out[...]


def pack(w_query, w_key, w_value, w_out):
    return pl.pallas_call(
        pack_body, out_shape=(bf(2, ROWS, COLS), bf(LAST + 1, ROWS, COLS)),
        in_specs=[VMEM] * 4, out_specs=(VMEM,) * 2, compiler_params=PARAMS, name="pack",
    )(w_query, w_key, w_value, jnp.transpose(w_out))


def norm_body(tokens, other, gain, late, early):
    core = lax.axis_index("sp") % 2
    widened_gain = gain[...]

    def normed(v):
        v = v.astype(jnp.float32)
        v = v * lax.rsqrt(jnp.mean(v * v, axis=-1, keepdims=True) + epsilon)
        return (v * widened_gain).astype(jnp.bfloat16)

    for b in range(BATCHES):
        mine = normed(tokens[core * BATCHES + b])
        theirs = normed(other[b])

        @pl.when(core == 1)
        def _():
            late[b] = mine
            early[b] = theirs

        @pl.when(core == 0)
        def _():
            late[b] = theirs
            early[b] = mine


def norm_rows(tokens, other, gain):
    shape = bf(BATCHES, PIECE, WIDTH)
    return pl.pallas_call(
        norm_body, out_shape=(shape, shape), in_specs=[VMEM] * 3, out_specs=(VMEM,) * 2,
        compiler_params=PARAMS, name="norm_rows",
    )(tokens, other, gain.reshape(1, WIDTH))


def row_copies(pieces, base, x_all, sems):
    t = lax.axis_index("tp")
    copies = []
    for d, piece in enumerate(pieces):
        at = pl.multiple_of(base + ((t + RING - d) % RING) * PIECE, PIECE)
        copies.append(pltpu.make_async_copy(piece, x_all.at[:, pl.ds(at, PIECE), :], sems.at[base // HALF, d]))
    return copies


def shard_copies(lines, first, count, w_all, sems, kind):
    core = lax.axis_index("sp") % 2
    copies = []
    for n, line in enumerate(lines):
        whose = core if n < RING else 1 - core
        for j in range(RING):
            at = pl.multiple_of(place_of(whose, j, n % RING, kind) * ROWS, ROWS)
            copies.append(
                pltpu.make_async_copy(
                    line.at[j, pl.ds(first, count)], w_all.at[pl.ds(first, count), pl.ds(at, ROWS), :],
                    sems.at[n * RING + j],
                )
            )
    return copies


def wide_pair_body(*refs):
    pieces, lines = refs[:4], refs[4:12]
    out, x_all, w_all, x_sems, w_sems = refs[12:]
    copies = row_copies(pieces, 0, x_all, x_sems) + shard_copies(lines, 0, 2, w_all, w_sems, 0)
    for c in copies:
        c.start()
    for c in copies:
        c.wait()
    for role in range(2):
        x = x_all[...].reshape(BATCHES * HALF, WIDTH)
        y = jnp.dot(x, w_all[role], preferred_element_type=jnp.float32)
        out[role] = y.astype(jnp.bfloat16).reshape(BATCHES, HALF, COLS)


def project_wide(pieces, lines):
    return pl.pallas_call(
        wide_pair_body, out_shape=bf(2, BATCHES, HALF, COLS), in_specs=[ANY] * 12, out_specs=VMEM,
        scratch_shapes=[
            pltpu.VMEM((BATCHES, HALF, WIDTH), jnp.bfloat16), pltpu.VMEM((2, WIDTH, COLS), jnp.bfloat16),
            pltpu.SemaphoreType.DMA((1, RING)), pltpu.SemaphoreType.DMA((32,)),
        ],
        compiler_params=PARAMS, name="project_wide",
    )(*pieces, *lines)


def matrix_copies(lines, first, count, w_all, sems):
    core = lax.axis_index("sp") % 2
    groups = [[] for _ in range(count)]
    for n, line in enumerate(lines):
        whose = core if n < RING else 1 - core
        for j in range(RING):
            at = pl.multiple_of(place_of(whose, j, n % RING, 0) * ROWS, ROWS)
            for m in range(count):
                groups[m].append(
                    pltpu.make_async_copy(
                        line.at[j, first + m], w_all.at[m, pl.ds(at, ROWS), :], sems.at[m, n * RING + j]
                    )
                )
    return groups


def project(x_all, w_all, m):
    x = x_all[...].reshape(BATCHES * SPAN, WIDTH)
    y = jnp.dot(x, w_all[m], preferred_element_type=jnp.float32)
    return y.astype(jnp.bfloat16).reshape(BATCHES, SPAN, COLS)


def staged(early, late, rest, first, count, x_all, w_all, x_sems, w_sems, work):
    rows = row_copies(early, 0, x_all, x_sems) + row_copies(late, HALF, x_all, x_sems)
    weights = matrix_copies(rest, first, count, w_all, w_sems)
    for c in rows + weights[0] + weights[1]:
        c.start()
    for c in rows:
        c.wait()
    for m in range(count):
        for c in weights[m]:
            c.wait()
        if m + 2 < count:
            for c in weights[m + 2]:
                c.start()
        work(m, project(x_all, w_all, m))


def near_pair_body(*refs):
    early, late, rest = refs[:4], refs[4:8], refs[8:16]
    near, near_tail, *scratch = refs[16:]

    def work(m, y):
        near[m // 2, m % 2] = y
        if m < 2:
            near_tail[m % 2, :, : HALOS[0]] = y[:, SPAN - HALOS[0] :]
        else:
            near_tail[m % 2, :, HALOS[0] :] = y[:, SPAN - HALOS[1] :]

    staged(early, late, rest, 0, NEAR, *scratch, work)


def query_body(*refs):
    early, late, rest = refs[:4], refs[4:8], refs[8:16]
    queries, *scratch = refs[16:]

    def work(m, y):
        queries[m] = y

    staged(early, late, rest, NEAR, GROUPS, *scratch, work)


def rest_scratch(count):
    return [
        pltpu.VMEM((BATCHES, SPAN, WIDTH), jnp.bfloat16), pltpu.VMEM((count, WIDTH, COLS), jnp.bfloat16),
        pltpu.SemaphoreType.DMA((2, RING)), pltpu.SemaphoreType.DMA((count, 32)),
    ]


def project_near(early, late, rest):
    return pl.pallas_call(
        near_pair_body,
        out_shape=(bf(2, 2, BATCHES, SPAN, COLS), bf(2, BATCHES, HALOS[0] + HALOS[1], COLS)),
        in_specs=[ANY] * 16, out_specs=(VMEM,) * 2, scratch_shapes=rest_scratch(NEAR),
        compiler_params=PARAMS, name="project_near",
    )(*early, *late, *rest)


def project_queries(early, late, rest):
    return pl.pallas_call(
        query_body, out_shape=bf(GROUPS, BATCHES, SPAN, COLS),
        in_specs=[ANY] * 16, out_specs=VMEM, scratch_shapes=rest_scratch(GROUPS),
        compiler_params=PARAMS, name="project_queries",
    )(*early, *late, *rest)


def bias_of(group, block):
    halo, dilation = HALOS[group], DILATIONS[group]
    dims = (BLOCK, BLOCK + halo)
    q = lax.broadcasted_iota(jnp.int32, dims, 0)
    k = lax.broadcasted_iota(jnp.int32, dims, 1)
    lag = q + halo - k
    start = (lax.axis_index("sp") // 2) * SPAN + block * BLOCK - halo
    seen = (lag >= 0) & (lag <= STEPS * dilation) & ((lag & (dilation - 1)) == 0) & (k + start >= 0)
    return jnp.where(seen, 0.0, -1e30).astype(jnp.float32)


def attend(items):
    scores = [
        lax.dot_general(q, k, (((1,), (1,)), ((), ())), preferred_element_type=jnp.float32) for q, k, _, _ in items
    ]
    lifts = []
    for s, (_, _, _, bias) in zip(scores, items):
        s = s * (1.0 / math.sqrt(HEAD_WIDTH)) + bias
        peak = jnp.max(s, axis=-1, keepdims=True)
        lifted = jnp.exp(s - peak)
        lifts.append((lifted.astype(jnp.bfloat16), peak, jnp.sum(lifted, axis=-1, keepdims=True)))
    outs = [jnp.dot(p, v, preferred_element_type=jnp.float32) for (p, _, _), (_, _, v, _) in zip(lifts, items)]
    return [(o / total, peak + jnp.log(total)) for o, (_, peak, total) in zip(outs, lifts)]


def joined(o1, l1, o2, l2):
    top = jnp.maximum(l1, l2)
    a, c = jnp.exp(l1 - top), jnp.exp(l2 - top)
    total = a + c
    return (a * o1 + c * o2) / total, top + jnp.log(total)


PLACES = [
    (b, h, slice(h * HEAD_WIDTH, (h + 1) * HEAD_WIDTH)) for b in range(BATCHES) for h in range(COLS // HEAD_WIDTH)
]


def wide_body(q, early, late, back_early, back_late, far_late, out, logs, held, sems):
    copies = [
        pltpu.make_async_copy(part, held.at[:, :, pl.ds(n * HALF, HALF)], sems.at[n])
        for n, part in enumerate((far_late, back_early, back_late, early, late))
    ]
    for c in copies:
        c.start()
    for c in copies:
        c.wait()
    for i in range(SPAN // BLOCK):
        rows = slice(i * BLOCK, (i + 1) * BLOCK)
        keys = slice(i * BLOCK, (i + 1) * BLOCK + HALOS[2])
        bias = bias_of(2, i)
        found = attend([(q[b, rows, cols], held[0, b, keys, cols], held[1, b, keys, cols], bias) for b, _, cols in PLACES])
        for (b, _, cols), (o, l) in zip(PLACES, found):
            out[b, rows, cols] = o
            logs[b, rows, cols] = jnp.broadcast_to(l, (BLOCK, HEAD_WIDTH))


def attend_wide(q, early, late, back_early, back_late, far_late):
    shape = jax.ShapeDtypeStruct((BATCHES, SPAN, COLS), jnp.float32)
    return pl.pallas_call(
        wide_body, out_shape=(shape, shape),
        in_specs=[pl.BlockSpec((pl.squeezed, BATCHES, SPAN, COLS), lambda i: (2, 0, 0, 0))] + [ANY] * 5,
        out_specs=(VMEM,) * 2, grid=(1,),
        scratch_shapes=[
            pltpu.VMEM((2, BATCHES, HALOS[2] + SPAN, COLS), jnp.bfloat16), pltpu.SemaphoreType.DMA((5,)),
        ],
        compiler_params=PARAMS, name="attend_wide",
    )(q, early, late, back_early, back_late, far_late)


def near_body(q, near, tail, other, logs, c0, c1, c2, c3, kept, sent, k0, k1, mixed, weights, sems):
    copies = [
        pltpu.make_async_copy(tail.at[:, :, pl.ds(0, HALOS[0])], k0.at[:, :, pl.ds(0, HALOS[0])], sems.at[0]),
        pltpu.make_async_copy(tail.at[:, :, pl.ds(HALOS[0], HALOS[1])], k1.at[:, :, pl.ds(0, HALOS[1])], sems.at[1]),
        pltpu.make_async_copy(near.at[0], k0.at[:, :, pl.ds(HALOS[0], SPAN)], sems.at[2]),
        pltpu.make_async_copy(near.at[1], k1.at[:, :, pl.ds(HALOS[1], SPAN)], sems.at[3]),
    ]
    for c in copies:
        c.start()
    for c in copies:
        c.wait()
    core, t = lax.axis_index("sp") % 2, lax.axis_index("tp")
    for i in range(SPAN // BLOCK):
        rows = slice(i * BLOCK, (i + 1) * BLOCK)
        biases = [bias_of(g, i) for g in range(2)]
        for some in (PLACES[:3], PLACES[3:]):
            items = []
            for g, held in enumerate((k0, k1)):
                keys = slice(i * BLOCK, (i + 1) * BLOCK + HALOS[g])
                items += [
                    (q[g, b, rows, cols], held[0, b, keys, cols], held[1, b, keys, cols], biases[g]) for b, _, cols in some
                ]
            found = attend(items)
            for n, (b, h, cols) in enumerate(some):
                o, l = joined(*found[n], *found[n + 3])
                o, l = joined(o, l, other[b, rows, cols], logs[b, rows, cols])
                mixed[b, rows, cols] = o.astype(jnp.bfloat16)
                weights[i, 2 * b + h : 2 * b + h + 1, :] = jnp.transpose(l)[0:1]
    kept[...] = weights[core]
    sent[...] = weights[1 - core]
    for d, out in enumerate((c0, c1, c2, c3)):
        for far in range(2):
            whose = core if far == 0 else 1 - core
            at = pl.multiple_of(whose * HALF + ((t + d) % RING) * PIECE, PIECE)
            out[far] = mixed[:, pl.ds(at, PIECE), :]


def attend_near(q, near, tail, other, logs):
    piece = bf(2, BATCHES, PIECE, COLS)
    line = jax.ShapeDtypeStruct((2 * BATCHES, BLOCK), jnp.float32)
    return pl.pallas_call(
        near_body, out_shape=(piece,) * 4 + (line,) * 2, grid=(1,),
        in_specs=[pl.BlockSpec((2, BATCHES, SPAN, COLS), lambda i: (0, 0, 0, 0)), ANY, ANY, VMEM, VMEM],
        out_specs=(VMEM,) * 6,
        scratch_shapes=[
            pltpu.VMEM((2, BATCHES, HALOS[0] + SPAN, COLS), jnp.bfloat16),
            pltpu.VMEM((2, BATCHES, HALOS[1] + SPAN, COLS), jnp.bfloat16),
            pltpu.VMEM((BATCHES, SPAN, COLS), jnp.bfloat16),
            pltpu.VMEM((2, 2 * BATCHES, BLOCK), jnp.float32),
            pltpu.SemaphoreType.DMA((4,)),
        ],
        compiler_params=PARAMS, name="attend_near",
    )(q, near, tail, other, logs)


def pick_body(a0, a1, a2, a3, out, sems):
    copies = [
        pltpu.make_async_copy(a.at[:, LAST], out.at[pl.ds(RING * e, RING)], sems.at[e])
        for e, a in enumerate((a0, a1, a2, a3))
    ]
    for c in copies:
        c.start()
    for c in copies:
        c.wait()


def pick(lines):
    return pl.pallas_call(
        pick_body, out_shape=bf(16, ROWS, COLS), in_specs=[ANY] * 4, out_specs=VMEM,
        scratch_shapes=[pltpu.SemaphoreType.DMA((4,))], compiler_params=PARAMS, name="pick",
    )(*lines)


def final_body(*refs):
    received, lines, ours, crossed = refs[:4], refs[4:12], refs[12:15], refs[15:18]
    keep, send, w_all, sems = refs[18:]
    core = lax.axis_index("sp") % 2
    part = WIDTH // RING
    half = BATCHES * PIECE
    count = part // ROWS
    copies = []
    for n in range(2 * RING):
        whose = core if n < RING else 1 - core
        others = ours if n < RING else crossed
        for j in range(RING):
            k = place_of(whose, j, n % RING, 0)
            at = n * RING + j
            copies.append(pltpu.make_async_copy(lines[n].at[j, LAST], w_all.at[0, k], sems.at[0, at]))
            for d, piece in enumerate(others, 1):
                source = piece.at[(n % RING) * RING + j]
                copies.append(pltpu.make_async_copy(source, w_all.at[d, k], sems.at[d, at]))
    for c in copies:
        c.start()
    for c in copies:
        c.wait()
    rows = [r[...].reshape(2 * half, COLS) for r in received]
    for n in range(RING):
        cols = slice(n * part, (n + 1) * part)
        acc = None
        for d in range(RING):
            block = w_all[d, n * count : (n + 1) * count].reshape(part, COLS)
            y = lax.dot_general(rows[d], block, (((1,), (1,)), ((), ())), preferred_element_type=jnp.float32)
            acc = y if acc is None else acc + y
        acc = acc.astype(jnp.bfloat16)
        keep[:, :, cols] = acc[:half].reshape(BATCHES, PIECE, part)
        send[:, :, cols] = acc[half:].reshape(BATCHES, PIECE, part)


def finish(received, lines, pieces, crossed):
    shape = bf(BATCHES, PIECE, WIDTH)
    return pl.pallas_call(
        final_body, out_shape=(shape, shape), in_specs=[VMEM] * 4 + [ANY] * 14, out_specs=(VMEM,) * 2,
        scratch_shapes=[
            pltpu.VMEM((RING, WIDTH // ROWS, ROWS, COLS), jnp.bfloat16), pltpu.SemaphoreType.DMA((RING, 32)),
        ],
        compiler_params=PARAMS, name="finish",
    )(*received, *lines, *pieces, *crossed)


def joined_cores(mine, theirs):
    core = lax.axis_index("sp") % 2
    return jnp.where(core == 0, jnp.concatenate((mine, theirs), 0), jnp.concatenate((theirs, mine), 0))


def merge_body(mine, theirs, out):
    core = lax.axis_index("sp") % 2
    out[pl.ds(core * BATCHES, BATCHES)] = mine[...]
    out[pl.ds((1 - core) * BATCHES, BATCHES)] = theirs[...]


def merged(mine, theirs):
    return pl.pallas_call(
        merge_body, out_shape=bf(2 * BATCHES, PIECE, WIDTH), in_specs=[VMEM] * 2, out_specs=VMEM,
        compiler_params=PARAMS, name="merge",
    )(mine, theirs)


def ring_of(a):
    came = {d: turned(a, d) for d in (1, 3, 2)}
    return [a, came[1], came[2], came[3]]


def spread(own, kind):
    near = {d: lax.ppermute(own, "sp", first_leg(d, kind)) for d in (1, 3, 2)}
    line = jnp.stack((own, near[1], near[2], near[3]))
    far = {d: lax.ppermute(line, "sp", second_leg(d, kind)) for d in (1, 3, 2)}
    lines = [line, far[1], far[2], far[3]]
    return lines + [swapped(a) for a in lines]


def layer(tokens, norm_gain, w_query, w_key, w_value, w_out):
    wide_own, rest_own = pack(w_query, w_key, w_value, w_out)

    core = lax.axis_index("sp") % 2
    tokens = jnp.transpose(tokens, (1, 0, 2))
    send = lax.dynamic_slice_in_dim(tokens, (1 - core) * BATCHES, BATCHES, 0)
    other = swapped(send)
    wide_lines = spread(wide_own, 0)
    late, early = norm_rows(tokens, other, norm_gain)
    late, early = ring_of(late), ring_of(early)
    rest = spread(rest_own, 0)

    wide_late = project_wide(late, wide_lines)
    far_late = from_behind(wide_late, 2)
    back_late = from_behind(wide_late, 1)
    wide_early = project_wide(early, wide_lines)
    back_early = from_behind(wide_early, 1)
    near, near_tail = project_near(early, late, rest)
    near_tail = from_behind(near_tail, 1)
    outs = ring_of(pick(rest[:RING]))[1:]
    queries = project_queries(early, late, rest)
    wide_out, wide_logs = attend_wide(queries, wide_early, wide_late, back_early, back_late, far_late)
    *combined, kept, sent = attend_near(queries, near, near_tail, wide_out, wide_logs)

    received = [combined[0]] + [turned(combined[d], d) for d in (1, 2, 3)]
    mixed_mine, mixed_sent = finish(received, rest, outs, [swapped(a) for a in outs])
    mixed = merged(mixed_mine, swapped(mixed_sent))

    log_weight = joined_cores(kept, swapped(sent)).reshape(2 * BATCHES, 2, BLOCK)
    return (jnp.transpose(mixed, (1, 0, 2)), jnp.transpose(log_weight, (2, 0, 1)))


def solution(mesh):
    in_specs = (
        P(("sp", "tp"), None, None),
        P(),
        P(None, "sp", "tp"),
        P(None, "sp", "tp"),
        P(None, "sp", "tp"),
        P("tp", "sp"),
    )
    out_specs = (P(("sp", "tp"), None, None), P("sp", None, "tp"))
    return jax.shard_map(layer, mesh=mesh, in_specs=in_specs, out_specs=out_specs, check_vma=False)
```

```python
import math

import jax
import jax.numpy as jnp
from jax import lax
from jax.experimental import pallas as pl
from jax.experimental.pallas import tpu as pltpu
from jax.sharding import PartitionSpec as P


GROUPS = 3
STEPS = 24
DILATIONS = (1, 4, 16)
HALOS = (32, 96, 384)
RING = 4
BATCHES = 3
PIECE = 32
SPAN = 256
HEAD_WIDTH = 128
COLS = 256
ROWS = 64
WIDTH = 2048
BLOCK = 128

epsilon = 1e-06


def chip(z, y, core):
    return (z % RING) * 8 + (y % RING) * 2 + core


def chips():
    return [(z, y, core) for z in range(RING) for y in range(RING) for core in range(2)]


def first_leg(shift, kind):
    def way(k):
        return k if kind == 0 else 0

    return [(chip(z, y, k), chip(z + shift * way(k), y + shift * (1 - way(k)), k)) for z, y, k in chips()]


def second_leg(shift, kind):
    def way(k):
        return k if kind == 0 else 0

    return [(chip(z, y, k), chip(z + shift * (1 - way(k)), y + shift * way(k), k)) for z, y, k in chips()]


SWAP = [(i, i ^ 1) for i in range(32)]


def swapped(a):
    return lax.ppermute(a, "sp", SWAP)


def turned(a, shift):
    return lax.ppermute(a, "tp", [(i, (i + shift) % RING) for i in range(RING)])


def from_behind(a, blocks):
    return lax.ppermute(a, "sp", [(i, i + 2 * blocks) for i in range(32 - 2 * blocks)])


def place_of(core, first, second, kind):
    s = lax.axis_index("sp")
    z, y = s // 8, (s // 2) % RING
    if kind == 0:
        up = jnp.where(core == 0, second, first)
        along = jnp.where(core == 0, first, second)
    else:
        up, along = second, first
    return ((z + RING - up) % RING) * 8 + ((y + RING - along) % RING) * 2 + core


ANY = pl.BlockSpec(memory_space=pl.ANY)
VMEM = pl.BlockSpec(memory_space=pltpu.VMEM)
PARAMS = pltpu.CompilerParams(vmem_limit_bytes=56 * 1024 * 1024)
HALF = SPAN // 2
NEAR = 4
LAST = NEAR + GROUPS


def bf(*dims):
    return jax.ShapeDtypeStruct(dims, jnp.bfloat16)


def pack_body(w_query, w_key, w_value, w_out, wide, rest):
    wide[0] = w_key[2]
    wide[1] = w_value[2]
    for g in range(2):
        rest[2 * g] = w_key[g]
        rest[2 * g + 1] = w_value[g]
    rest[NEAR:LAST] = w_query[...]
    rest[LAST] = w_out[...]


def pack(w_query, w_key, w_value, w_out):
    return pl.pallas_call(
        pack_body, out_shape=(bf(2, ROWS, COLS), bf(LAST + 1, ROWS, COLS)),
        in_specs=[VMEM] * 4, out_specs=(VMEM,) * 2, compiler_params=PARAMS, name="pack",
    )(w_query, w_key, w_value, jnp.transpose(w_out))


def norm_body(tokens, other, gain, late, early):
    core = lax.axis_index("sp") % 2
    widened_gain = gain[...]

    def normed(v):
        v = v.astype(jnp.float32)
        v = v * lax.rsqrt(jnp.mean(v * v, axis=-1, keepdims=True) + epsilon)
        return (v * widened_gain).astype(jnp.bfloat16)

    for b in range(BATCHES):
        mine = normed(tokens[core * BATCHES + b])
        theirs = normed(other[b])

        @pl.when(core == 1)
        def _():
            late[b] = mine
            early[b] = theirs

        @pl.when(core == 0)
        def _():
            late[b] = theirs
            early[b] = mine


def norm_rows(tokens, other, gain):
    shape = bf(BATCHES, PIECE, WIDTH)
    return pl.pallas_call(
        norm_body, out_shape=(shape, shape), in_specs=[VMEM] * 3, out_specs=(VMEM,) * 2,
        compiler_params=PARAMS, name="norm_rows",
    )(tokens, other, gain.reshape(1, WIDTH))


def row_copies(pieces, base, x_all, sems):
    t = lax.axis_index("tp")
    copies = []
    for d, piece in enumerate(pieces):
        at = pl.multiple_of(base + ((t + RING - d) % RING) * PIECE, PIECE)
        copies.append(pltpu.make_async_copy(piece, x_all.at[:, pl.ds(at, PIECE), :], sems.at[base // HALF, d]))
    return copies


def shard_copies(lines, first, count, w_all, sems, kind):
    core = lax.axis_index("sp") % 2
    copies = []
    for n, line in enumerate(lines):
        whose = core if n < RING else 1 - core
        for j in range(RING):
            at = pl.multiple_of(place_of(whose, j, n % RING, kind) * ROWS, ROWS)
            copies.append(
                pltpu.make_async_copy(
                    line.at[j, pl.ds(first, count)], w_all.at[pl.ds(first, count), pl.ds(at, ROWS), :],
                    sems.at[n * RING + j],
                )
            )
    return copies


def wide_pair_body(*refs):
    pieces, lines = refs[:4], refs[4:12]
    out, x_all, w_all, x_sems, w_sems = refs[12:]
    copies = row_copies(pieces, 0, x_all, x_sems) + shard_copies(lines, 0, 2, w_all, w_sems, 0)
    for c in copies:
        c.start()
    for c in copies:
        c.wait()
    for role in range(2):
        x = x_all[...].reshape(BATCHES * HALF, WIDTH)
        y = jnp.dot(x, w_all[role], preferred_element_type=jnp.float32)
        out[role] = y.astype(jnp.bfloat16).reshape(BATCHES, HALF, COLS)


def project_wide(pieces, lines):
    return pl.pallas_call(
        wide_pair_body, out_shape=bf(2, BATCHES, HALF, COLS), in_specs=[ANY] * 12, out_specs=VMEM,
        scratch_shapes=[
            pltpu.VMEM((BATCHES, HALF, WIDTH), jnp.bfloat16), pltpu.VMEM((2, WIDTH, COLS), jnp.bfloat16),
            pltpu.SemaphoreType.DMA((1, RING)), pltpu.SemaphoreType.DMA((32,)),
        ],
        compiler_params=PARAMS, name="project_wide",
    )(*pieces, *lines)


def matrix_copies(lines, first, count, w_all, sems):
    core = lax.axis_index("sp") % 2
    groups = [[] for _ in range(count)]
    for n, line in enumerate(lines):
        whose = core if n < RING else 1 - core
        for j in range(RING):
            at = pl.multiple_of(place_of(whose, j, n % RING, 0) * ROWS, ROWS)
            for m in range(count):
                groups[m].append(
                    pltpu.make_async_copy(
                        line.at[j, first + m], w_all.at[m, pl.ds(at, ROWS), :], sems.at[m, n * RING + j]
                    )
                )
    return groups


def project(x_all, w_all, m):
    x = x_all[...].reshape(BATCHES * SPAN, WIDTH)
    y = jnp.dot(x, w_all[m], preferred_element_type=jnp.float32)
    return y.astype(jnp.bfloat16).reshape(BATCHES, SPAN, COLS)


def staged(early, late, rest, first, count, x_all, w_all, x_sems, w_sems, work):
    rows = row_copies(early, 0, x_all, x_sems) + row_copies(late, HALF, x_all, x_sems)
    weights = matrix_copies(rest, first, count, w_all, w_sems)
    for c in rows + weights[0] + weights[1]:
        c.start()
    for c in rows:
        c.wait()
    for m in range(count):
        for c in weights[m]:
            c.wait()
        if m + 2 < count:
            for c in weights[m + 2]:
                c.start()
        work(m, project(x_all, w_all, m))


def near_pair_body(*refs):
    early, late, rest = refs[:4], refs[4:8], refs[8:16]
    near, near_tail, *scratch = refs[16:]

    def work(m, y):
        near[m // 2, m % 2] = y
        if m < 2:
            near_tail[m % 2, :, : HALOS[0]] = y[:, SPAN - HALOS[0] :]
        else:
            near_tail[m % 2, :, HALOS[0] :] = y[:, SPAN - HALOS[1] :]

    staged(early, late, rest, 0, NEAR, *scratch, work)


def query_body(*refs):
    early, late, rest = refs[:4], refs[4:8], refs[8:16]
    queries, *scratch = refs[16:]

    def work(m, y):
        queries[m] = y

    staged(early, late, rest, 0, GROUPS, *scratch, work)


def rest_scratch(count):
    return [
        pltpu.VMEM((BATCHES, SPAN, WIDTH), jnp.bfloat16), pltpu.VMEM((count, WIDTH, COLS), jnp.bfloat16),
        pltpu.SemaphoreType.DMA((2, RING)), pltpu.SemaphoreType.DMA((count, 32)),
    ]


def project_near(early, late, rest):
    return pl.pallas_call(
        near_pair_body,
        out_shape=(bf(2, 2, BATCHES, SPAN, COLS), bf(2, BATCHES, HALOS[0] + HALOS[1], COLS)),
        in_specs=[ANY] * 16, out_specs=(VMEM,) * 2, scratch_shapes=rest_scratch(NEAR),
        compiler_params=PARAMS, name="project_near",
    )(*early, *late, *rest)


def project_queries(early, late, rest):
    return pl.pallas_call(
        query_body, out_shape=bf(GROUPS, BATCHES, SPAN, COLS),
        in_specs=[ANY] * 16, out_specs=VMEM, scratch_shapes=rest_scratch(GROUPS),
        compiler_params=PARAMS, name="project_queries",
    )(*early, *late, *rest)


def bias_of(group, block):
    halo, dilation = HALOS[group], DILATIONS[group]
    dims = (BLOCK, BLOCK + halo)
    q = lax.broadcasted_iota(jnp.int32, dims, 0)
    k = lax.broadcasted_iota(jnp.int32, dims, 1)
    lag = q + halo - k
    start = (lax.axis_index("sp") // 2) * SPAN + block * BLOCK - halo
    seen = (lag >= 0) & (lag <= STEPS * dilation) & ((lag & (dilation - 1)) == 0) & (k + start >= 0)
    return jnp.where(seen, 0.0, -1e30).astype(jnp.float32)


def attend(items):
    scores = [
        lax.dot_general(q, k, (((1,), (1,)), ((), ())), preferred_element_type=jnp.float32) for q, k, _, _ in items
    ]
    lifts = []
    for s, (_, _, _, bias) in zip(scores, items):
        s = s * (1.0 / math.sqrt(HEAD_WIDTH)) + bias
        peak = jnp.max(s, axis=-1, keepdims=True)
        lifted = jnp.exp(s - peak)
        lifts.append((lifted.astype(jnp.bfloat16), peak, jnp.sum(lifted, axis=-1, keepdims=True)))
    outs = [jnp.dot(p, v, preferred_element_type=jnp.float32) for (p, _, _), (_, _, v, _) in zip(lifts, items)]
    return [(o / total, peak + jnp.log(total)) for o, (_, peak, total) in zip(outs, lifts)]


def joined(o1, l1, o2, l2):
    top = jnp.maximum(l1, l2)
    a, c = jnp.exp(l1 - top), jnp.exp(l2 - top)
    total = a + c
    return (a * o1 + c * o2) / total, top + jnp.log(total)


PLACES = [
    (b, h, slice(h * HEAD_WIDTH, (h + 1) * HEAD_WIDTH)) for b in range(BATCHES) for h in range(COLS // HEAD_WIDTH)
]


def wide_body(q, early, late, back_early, back_late, far_late, out, logs, held, sems):
    copies = [
        pltpu.make_async_copy(part, held.at[:, :, pl.ds(n * HALF, HALF)], sems.at[n])
        for n, part in enumerate((far_late, back_early, back_late, early, late))
    ]
    for c in copies:
        c.start()
    for c in copies:
        c.wait()
    for i in range(SPAN // BLOCK):
        rows = slice(i * BLOCK, (i + 1) * BLOCK)
        keys = slice(i * BLOCK, (i + 1) * BLOCK + HALOS[2])
        bias = bias_of(2, i)
        found = attend([(q[b, rows, cols], held[0, b, keys, cols], held[1, b, keys, cols], bias) for b, _, cols in PLACES])
        for (b, _, cols), (o, l) in zip(PLACES, found):
            out[b, rows, cols] = o
            logs[b, rows, cols] = jnp.broadcast_to(l, (BLOCK, HEAD_WIDTH))


def attend_wide(q, early, late, back_early, back_late, far_late):
    shape = jax.ShapeDtypeStruct((BATCHES, SPAN, COLS), jnp.float32)
    return pl.pallas_call(
        wide_body, out_shape=(shape, shape),
        in_specs=[pl.BlockSpec((pl.squeezed, BATCHES, SPAN, COLS), lambda i: (2, 0, 0, 0))] + [ANY] * 5,
        out_specs=(VMEM,) * 2, grid=(1,),
        scratch_shapes=[
            pltpu.VMEM((2, BATCHES, HALOS[2] + SPAN, COLS), jnp.bfloat16), pltpu.SemaphoreType.DMA((5,)),
        ],
        compiler_params=PARAMS, name="attend_wide",
    )(q, early, late, back_early, back_late, far_late)


def near_body(q, near, tail, other, logs, c0, c1, c2, c3, kept, sent, k0, k1, mixed, weights, sems):
    copies = [
        pltpu.make_async_copy(tail.at[:, :, pl.ds(0, HALOS[0])], k0.at[:, :, pl.ds(0, HALOS[0])], sems.at[0]),
        pltpu.make_async_copy(tail.at[:, :, pl.ds(HALOS[0], HALOS[1])], k1.at[:, :, pl.ds(0, HALOS[1])], sems.at[1]),
        pltpu.make_async_copy(near.at[0], k0.at[:, :, pl.ds(HALOS[0], SPAN)], sems.at[2]),
        pltpu.make_async_copy(near.at[1], k1.at[:, :, pl.ds(HALOS[1], SPAN)], sems.at[3]),
    ]
    for c in copies:
        c.start()
    for c in copies:
        c.wait()
    core, t = lax.axis_index("sp") % 2, lax.axis_index("tp")
    for i in range(SPAN // BLOCK):
        rows = slice(i * BLOCK, (i + 1) * BLOCK)
        biases = [bias_of(g, i) for g in range(2)]
        for some in (PLACES[:3], PLACES[3:]):
            items = []
            for g, held in enumerate((k0, k1)):
                keys = slice(i * BLOCK, (i + 1) * BLOCK + HALOS[g])
                items += [
                    (q[g, b, rows, cols], held[0, b, keys, cols], held[1, b, keys, cols], biases[g]) for b, _, cols in some
                ]
            found = attend(items)
            for n, (b, h, cols) in enumerate(some):
                o, l = joined(*found[n], *found[n + 3])
                o, l = joined(o, l, other[b, rows, cols], logs[b, rows, cols])
                mixed[b, rows, cols] = o.astype(jnp.bfloat16)
                weights[i, 2 * b + h : 2 * b + h + 1, :] = jnp.transpose(l)[0:1]
    kept[...] = weights[core]
    sent[...] = weights[1 - core]
    for d, out in enumerate((c0, c1, c2, c3)):
        for far in range(2):
            whose = core if far == 0 else 1 - core
            at = pl.multiple_of(whose * HALF + ((t + d) % RING) * PIECE, PIECE)
            out[far] = mixed[:, pl.ds(at, PIECE), :]


def attend_near(q, near, tail, other, logs):
    piece = bf(2, BATCHES, PIECE, COLS)
    line = jax.ShapeDtypeStruct((2 * BATCHES, BLOCK), jnp.float32)
    return pl.pallas_call(
        near_body, out_shape=(piece,) * 4 + (line,) * 2, grid=(1,),
        in_specs=[pl.BlockSpec((2, BATCHES, SPAN, COLS), lambda i: (0, 0, 0, 0)), ANY, ANY, VMEM, VMEM],
        out_specs=(VMEM,) * 6,
        scratch_shapes=[
            pltpu.VMEM((2, BATCHES, HALOS[0] + SPAN, COLS), jnp.bfloat16),
            pltpu.VMEM((2, BATCHES, HALOS[1] + SPAN, COLS), jnp.bfloat16),
            pltpu.VMEM((BATCHES, SPAN, COLS), jnp.bfloat16),
            pltpu.VMEM((2, 2 * BATCHES, BLOCK), jnp.float32),
            pltpu.SemaphoreType.DMA((4,)),
        ],
        compiler_params=PARAMS, name="attend_near",
    )(q, near, tail, other, logs)


def pick_body(a0, a1, a2, a3, out, sems):
    copies = [
        pltpu.make_async_copy(a.at[:, GROUPS], out.at[pl.ds(RING * e, RING)], sems.at[e])
        for e, a in enumerate((a0, a1, a2, a3))
    ]
    for c in copies:
        c.start()
    for c in copies:
        c.wait()


def pick(lines):
    return pl.pallas_call(
        pick_body, out_shape=bf(16, ROWS, COLS), in_specs=[ANY] * 4, out_specs=VMEM,
        scratch_shapes=[pltpu.SemaphoreType.DMA((4,))], compiler_params=PARAMS, name="pick",
    )(*lines)


def final_body(*refs):
    received, lines, ours, crossed = refs[:4], refs[4:12], refs[12:15], refs[15:18]
    keep, send, w_all, sems = refs[18:]
    core = lax.axis_index("sp") % 2
    part = WIDTH // RING
    half = BATCHES * PIECE
    count = part // ROWS
    copies = []
    for n in range(2 * RING):
        whose = core if n < RING else 1 - core
        others = ours if n < RING else crossed
        for j in range(RING):
            k = place_of(whose, j, n % RING, 0)
            at = n * RING + j
            copies.append(pltpu.make_async_copy(lines[n].at[j, GROUPS], w_all.at[0, k], sems.at[0, at]))
            for d, piece in enumerate(others, 1):
                source = piece.at[(n % RING) * RING + j]
                copies.append(pltpu.make_async_copy(source, w_all.at[d, k], sems.at[d, at]))
    for c in copies:
        c.start()
    for c in copies:
        c.wait()
    rows = [r[...].reshape(2 * half, COLS) for r in received]
    for n in range(RING):
        cols = slice(n * part, (n + 1) * part)
        acc = None
        for d in range(RING):
            block = w_all[d, n * count : (n + 1) * count].reshape(part, COLS)
            y = lax.dot_general(rows[d], block, (((1,), (1,)), ((), ())), preferred_element_type=jnp.float32)
            acc = y if acc is None else acc + y
        acc = acc.astype(jnp.bfloat16)
        keep[:, :, cols] = acc[:half].reshape(BATCHES, PIECE, part)
        send[:, :, cols] = acc[half:].reshape(BATCHES, PIECE, part)


def finish(received, lines, pieces, crossed):
    shape = bf(BATCHES, PIECE, WIDTH)
    return pl.pallas_call(
        final_body, out_shape=(shape, shape), in_specs=[VMEM] * 4 + [ANY] * 14, out_specs=(VMEM,) * 2,
        scratch_shapes=[
            pltpu.VMEM((RING, WIDTH // ROWS, ROWS, COLS), jnp.bfloat16), pltpu.SemaphoreType.DMA((RING, 32)),
        ],
        compiler_params=PARAMS, name="finish",
    )(*received, *lines, *pieces, *crossed)


def joined_cores(mine, theirs):
    core = lax.axis_index("sp") % 2
    return jnp.where(core == 0, jnp.concatenate((mine, theirs), 0), jnp.concatenate((theirs, mine), 0))


def merge_body(mine, theirs, out):
    core = lax.axis_index("sp") % 2
    out[pl.ds(core * BATCHES, BATCHES)] = mine[...]
    out[pl.ds((1 - core) * BATCHES, BATCHES)] = theirs[...]


def merged(mine, theirs):
    return pl.pallas_call(
        merge_body, out_shape=bf(2 * BATCHES, PIECE, WIDTH), in_specs=[VMEM] * 2, out_specs=VMEM,
        compiler_params=PARAMS, name="merge",
    )(mine, theirs)


def ring_of(a):
    came = {d: turned(a, d) for d in (1, 3, 2)}
    return [a, came[1], came[2], came[3]]


def spread(own, kind):
    near = {d: lax.ppermute(own, "sp", first_leg(d, kind)) for d in (1, 3, 2)}
    line = jnp.stack((own, near[1], near[2], near[3]))
    far = {d: lax.ppermute(line, "sp", second_leg(d, kind)) for d in (1, 3, 2)}
    lines = [line, far[1], far[2], far[3]]
    return lines + [swapped(a) for a in lines]


def spread_halves(own):
    near = {d: lax.ppermute(own, "sp", first_leg(d, 0)) for d in (1, 3, 2)}
    halves = []
    for part, way in ((slice(0, NEAR), 1), (slice(NEAR, None), 3)):
        line = jnp.stack([a[part] for a in (own, near[1], near[2], near[3])])
        far = {d: lax.ppermute(line, "sp", second_leg(d, 0)) for d in (1, 3)}
        far[2] = lax.ppermute(far[way], "sp", second_leg(way, 0))
        lines = [line, far[1], far[2], far[3]]
        halves.append(lines + [swapped(a) for a in lines])
    return halves


def layer(tokens, norm_gain, w_query, w_key, w_value, w_out):
    wide_own, rest_own = pack(w_query, w_key, w_value, w_out)

    core = lax.axis_index("sp") % 2
    tokens = jnp.transpose(tokens, (1, 0, 2))
    send = lax.dynamic_slice_in_dim(tokens, (1 - core) * BATCHES, BATCHES, 0)
    other = swapped(send)
    wide_lines = spread(wide_own, 0)
    late, early = norm_rows(tokens, other, norm_gain)
    late, early = ring_of(late), ring_of(early)
    pair_lines, query_lines = spread_halves(rest_own)

    wide_late = project_wide(late, wide_lines)
    far_late = from_behind(wide_late, 2)
    back_late = from_behind(wide_late, 1)
    wide_early = project_wide(early, wide_lines)
    back_early = from_behind(wide_early, 1)
    near, near_tail = project_near(early, late, pair_lines)
    near_tail = from_behind(near_tail, 1)
    outs = ring_of(pick(query_lines[:RING]))[1:]
    queries = project_queries(early, late, query_lines)
    wide_out, wide_logs = attend_wide(queries, wide_early, wide_late, back_early, back_late, far_late)
    *combined, kept, sent = attend_near(queries, near, near_tail, wide_out, wide_logs)

    received = [combined[0]] + [turned(combined[d], d) for d in (1, 2, 3)]
    mixed_mine, mixed_sent = finish(received, query_lines, outs, [swapped(a) for a in outs])
    mixed = merged(mixed_mine, swapped(mixed_sent))

    log_weight = joined_cores(kept, swapped(sent)).reshape(2 * BATCHES, 2, BLOCK)
    return (jnp.transpose(mixed, (1, 0, 2)), jnp.transpose(log_weight, (2, 0, 1)))


def solution(mesh):
    in_specs = (
        P(("sp", "tp"), None, None),
        P(),
        P(None, "sp", "tp"),
        P(None, "sp", "tp"),
        P(None, "sp", "tp"),
        P("tp", "sp"),
    )
    out_specs = (P(("sp", "tp"), None, None), P("sp", None, "tp"))
    return jax.shard_map(layer, mesh=mesh, in_specs=in_specs, out_specs=out_specs, check_vma=False)
```

```python
import math

import jax
import jax.numpy as jnp
from jax import lax
from jax.experimental import pallas as pl
from jax.experimental.pallas import tpu as pltpu
from jax.sharding import PartitionSpec as P


GROUPS = 3
STEPS = 24
DILATIONS = (1, 4, 16)
HALOS = (32, 96, 384)
RING = 4
BATCHES = 3
PIECE = 32
SPAN = 256
HEAD_WIDTH = 128
COLS = 256
ROWS = 64
WIDTH = 2048
BLOCK = 128

epsilon = 1e-06


def chip(z, y, core):
    return (z % RING) * 8 + (y % RING) * 2 + core


def chips():
    return [(z, y, core) for z in range(RING) for y in range(RING) for core in range(2)]


def first_leg(shift, kind):
    def way(k):
        return k if kind == 0 else 0

    return [(chip(z, y, k), chip(z + shift * way(k), y + shift * (1 - way(k)), k)) for z, y, k in chips()]


def second_leg(shift, kind):
    def way(k):
        return k if kind == 0 else 0

    return [(chip(z, y, k), chip(z + shift * (1 - way(k)), y + shift * way(k), k)) for z, y, k in chips()]


SWAP = [(i, i ^ 1) for i in range(32)]


def swapped(a):
    return lax.ppermute(a, "sp", SWAP)


def turned(a, shift):
    return lax.ppermute(a, "tp", [(i, (i + shift) % RING) for i in range(RING)])


def from_behind(a, blocks):
    return lax.ppermute(a, "sp", [(i, i + 2 * blocks) for i in range(32 - 2 * blocks)])


def place_of(core, first, second, kind):
    s = lax.axis_index("sp")
    z, y = s // 8, (s // 2) % RING
    if kind == 0:
        up = jnp.where(core == 0, second, first)
        along = jnp.where(core == 0, first, second)
    else:
        up, along = second, first
    return ((z + RING - up) % RING) * 8 + ((y + RING - along) % RING) * 2 + core


ANY = pl.BlockSpec(memory_space=pl.ANY)
VMEM = pl.BlockSpec(memory_space=pltpu.VMEM)
PARAMS = pltpu.CompilerParams(vmem_limit_bytes=56 * 1024 * 1024)
HALF = SPAN // 2
NEAR = 4
LAST = NEAR + GROUPS


def bf(*dims):
    return jax.ShapeDtypeStruct(dims, jnp.bfloat16)


def pack_body(w_query, w_key, w_value, w_out, wide, rest):
    wide[0] = w_key[2]
    wide[1] = w_value[2]
    for g in range(2):
        rest[2 * g] = w_key[g]
        rest[2 * g + 1] = w_value[g]
    rest[NEAR:LAST] = w_query[...]
    rest[LAST] = w_out[...]


def pack(w_query, w_key, w_value, w_out):
    return pl.pallas_call(
        pack_body, out_shape=(bf(2, ROWS, COLS), bf(LAST + 1, ROWS, COLS)),
        in_specs=[VMEM] * 4, out_specs=(VMEM,) * 2, compiler_params=PARAMS, name="pack",
    )(w_query, w_key, w_value, jnp.transpose(w_out))


def norm_body(tokens, other, gain, late, early):
    core = lax.axis_index("sp") % 2
    widened_gain = gain[...]

    def normed(v):
        v = v.astype(jnp.float32)
        v = v * lax.rsqrt(jnp.mean(v * v, axis=-1, keepdims=True) + epsilon)
        return (v * widened_gain).astype(jnp.bfloat16)

    for b in range(BATCHES):
        mine = normed(tokens[core * BATCHES + b])
        theirs = normed(other[b])

        @pl.when(core == 1)
        def _():
            late[b] = mine
            early[b] = theirs

        @pl.when(core == 0)
        def _():
            late[b] = theirs
            early[b] = mine


def norm_rows(tokens, other, gain):
    shape = bf(BATCHES, PIECE, WIDTH)
    return pl.pallas_call(
        norm_body, out_shape=(shape, shape), in_specs=[VMEM] * 3, out_specs=(VMEM,) * 2,
        compiler_params=PARAMS, name="norm_rows",
    )(tokens, other, gain.reshape(1, WIDTH))


def row_copies(pieces, base, x_all, sems):
    t = lax.axis_index("tp")
    copies = []
    for d, piece in enumerate(pieces):
        at = pl.multiple_of(base + ((t + RING - d) % RING) * PIECE, PIECE)
        copies.append(pltpu.make_async_copy(piece, x_all.at[:, pl.ds(at, PIECE), :], sems.at[base // HALF, d]))
    return copies


def shard_copies(lines, first, count, w_all, sems, kind):
    core = lax.axis_index("sp") % 2
    copies = []
    for n, line in enumerate(lines):
        whose = core if n < RING else 1 - core
        for j in range(RING):
            at = pl.multiple_of(place_of(whose, j, n % RING, kind) * ROWS, ROWS)
            copies.append(
                pltpu.make_async_copy(
                    line.at[j, pl.ds(first, count)], w_all.at[pl.ds(first, count), pl.ds(at, ROWS), :],
                    sems.at[n * RING + j],
                )
            )
    return copies


def wide_pair_body(*refs):
    pieces, lines = refs[:4], refs[4:12]
    out, x_all, w_all, x_sems, w_sems = refs[12:]
    copies = row_copies(pieces, 0, x_all, x_sems) + shard_copies(lines, 0, 2, w_all, w_sems, 0)
    for c in copies:
        c.start()
    for c in copies:
        c.wait()
    for role in range(2):
        x = x_all[...].reshape(BATCHES * HALF, WIDTH)
        y = jnp.dot(x, w_all[role], preferred_element_type=jnp.float32)
        out[role] = y.astype(jnp.bfloat16).reshape(BATCHES, HALF, COLS)


def project_wide(pieces, lines):
    return pl.pallas_call(
        wide_pair_body, out_shape=bf(2, BATCHES, HALF, COLS), in_specs=[ANY] * 12, out_specs=VMEM,
        scratch_shapes=[
            pltpu.VMEM((BATCHES, HALF, WIDTH), jnp.bfloat16), pltpu.VMEM((2, WIDTH, COLS), jnp.bfloat16),
            pltpu.SemaphoreType.DMA((1, RING)), pltpu.SemaphoreType.DMA((32,)),
        ],
        compiler_params=PARAMS, name="project_wide",
    )(*pieces, *lines)


def project(x_all, w_all, m):
    x = x_all[...].reshape(BATCHES * SPAN, WIDTH)
    y = jnp.dot(x, w_all[m], preferred_element_type=jnp.float32)
    return y.astype(jnp.bfloat16).reshape(BATCHES, SPAN, COLS)


def staged(early, late, lines, parts, x_all, w_all, x_sems, w_sems, work):
    rows = row_copies(early, 0, x_all, x_sems) + row_copies(late, HALF, x_all, x_sems)
    weights = [shard_copies(lines, first, count, w_all, w_sems.at[n], 0) for n, (first, count) in enumerate(parts)]
    for c in rows + weights[0]:
        c.start()
    for c in rows:
        c.wait()
    for n, (first, count) in enumerate(parts):
        for c in weights[n]:
            c.wait()
        if n + 1 < len(parts):
            for c in weights[n + 1]:
                c.start()
        for m in range(first, first + count):
            work(m, project(x_all, w_all, m))


def near_pair_body(*refs):
    early, late, rest = refs[:4], refs[4:8], refs[8:16]
    near, near_tail, *scratch = refs[16:]

    def work(m, y):
        near[m // 2, m % 2] = y
        if m < 2:
            near_tail[m % 2, :, : HALOS[0]] = y[:, SPAN - HALOS[0] :]
        else:
            near_tail[m % 2, :, HALOS[0] :] = y[:, SPAN - HALOS[1] :]

    staged(early, late, rest, ((0, 2), (2, 2)), *scratch, work)


def query_body(*refs):
    early, late, rest = refs[:4], refs[4:8], refs[8:16]
    queries, *scratch = refs[16:]

    def work(m, y):
        queries[m] = y

    staged(early, late, rest, ((0, 1), (1, 2)), *scratch, work)


def rest_scratch(count):
    return [
        pltpu.VMEM((BATCHES, SPAN, WIDTH), jnp.bfloat16), pltpu.VMEM((count, WIDTH, COLS), jnp.bfloat16),
        pltpu.SemaphoreType.DMA((2, RING)), pltpu.SemaphoreType.DMA((2, 32)),
    ]


def project_near(early, late, rest):
    return pl.pallas_call(
        near_pair_body,
        out_shape=(bf(2, 2, BATCHES, SPAN, COLS), bf(2, BATCHES, HALOS[0] + HALOS[1], COLS)),
        in_specs=[ANY] * 16, out_specs=(VMEM,) * 2, scratch_shapes=rest_scratch(NEAR),
        compiler_params=PARAMS, name="project_near",
    )(*early, *late, *rest)


def project_queries(early, late, rest):
    return pl.pallas_call(
        query_body, out_shape=bf(GROUPS, BATCHES, SPAN, COLS),
        in_specs=[ANY] * 16, out_specs=VMEM, scratch_shapes=rest_scratch(GROUPS),
        compiler_params=PARAMS, name="project_queries",
    )(*early, *late, *rest)


def bias_of(group, block):
    halo, dilation = HALOS[group], DILATIONS[group]
    dims = (BLOCK, BLOCK + halo)
    q = lax.broadcasted_iota(jnp.int32, dims, 0)
    k = lax.broadcasted_iota(jnp.int32, dims, 1)
    lag = q + halo - k
    start = (lax.axis_index("sp") // 2) * SPAN + block * BLOCK - halo
    seen = (lag >= 0) & (lag <= STEPS * dilation) & ((lag & (dilation - 1)) == 0) & (k + start >= 0)
    return jnp.where(seen, 0.0, -1e30).astype(jnp.float32)


def attend(items):
    scores = [
        lax.dot_general(q, k, (((1,), (1,)), ((), ())), preferred_element_type=jnp.float32) for q, k, _, _ in items
    ]
    lifts = []
    for s, (_, _, _, bias) in zip(scores, items):
        s = s * (1.0 / math.sqrt(HEAD_WIDTH)) + bias
        peak = jnp.max(s, axis=-1, keepdims=True)
        lifted = jnp.exp(s - peak)
        lifts.append((lifted.astype(jnp.bfloat16), peak, jnp.sum(lifted, axis=-1, keepdims=True)))
    outs = [jnp.dot(p, v, preferred_element_type=jnp.float32) for (p, _, _), (_, _, v, _) in zip(lifts, items)]
    return [(o / total, peak + jnp.log(total)) for o, (_, peak, total) in zip(outs, lifts)]


def joined(o1, l1, o2, l2):
    top = jnp.maximum(l1, l2)
    a, c = jnp.exp(l1 - top), jnp.exp(l2 - top)
    total = a + c
    return (a * o1 + c * o2) / total, top + jnp.log(total)


PLACES = [
    (b, h, slice(h * HEAD_WIDTH, (h + 1) * HEAD_WIDTH)) for b in range(BATCHES) for h in range(COLS // HEAD_WIDTH)
]


def wide_body(q, early, late, back_early, back_late, far_late, out, logs, held, sems):
    copies = [
        pltpu.make_async_copy(part, held.at[:, :, pl.ds(n * HALF, HALF)], sems.at[n])
        for n, part in enumerate((far_late, back_early, back_late, early, late))
    ]
    for c in copies:
        c.start()
    for c in copies:
        c.wait()
    for i in range(SPAN // BLOCK):
        rows = slice(i * BLOCK, (i + 1) * BLOCK)
        keys = slice(i * BLOCK, (i + 1) * BLOCK + HALOS[2])
        bias = bias_of(2, i)
        found = attend([(q[b, rows, cols], held[0, b, keys, cols], held[1, b, keys, cols], bias) for b, _, cols in PLACES])
        for (b, _, cols), (o, l) in zip(PLACES, found):
            out[b, rows, cols] = o
            logs[b, rows, cols] = jnp.broadcast_to(l, (BLOCK, HEAD_WIDTH))


def attend_wide(q, early, late, back_early, back_late, far_late):
    shape = jax.ShapeDtypeStruct((BATCHES, SPAN, COLS), jnp.float32)
    return pl.pallas_call(
        wide_body, out_shape=(shape, shape),
        in_specs=[pl.BlockSpec((pl.squeezed, BATCHES, SPAN, COLS), lambda i: (2, 0, 0, 0))] + [ANY] * 5,
        out_specs=(VMEM,) * 2, grid=(1,),
        scratch_shapes=[
            pltpu.VMEM((2, BATCHES, HALOS[2] + SPAN, COLS), jnp.bfloat16), pltpu.SemaphoreType.DMA((5,)),
        ],
        compiler_params=PARAMS, name="attend_wide",
    )(q, early, late, back_early, back_late, far_late)


def near_body(q, near, tail, other, logs, c0, c1, c2, c3, kept, sent, k0, k1, mixed, weights, sems):
    copies = [
        pltpu.make_async_copy(tail.at[:, :, pl.ds(0, HALOS[0])], k0.at[:, :, pl.ds(0, HALOS[0])], sems.at[0]),
        pltpu.make_async_copy(tail.at[:, :, pl.ds(HALOS[0], HALOS[1])], k1.at[:, :, pl.ds(0, HALOS[1])], sems.at[1]),
        pltpu.make_async_copy(near.at[0], k0.at[:, :, pl.ds(HALOS[0], SPAN)], sems.at[2]),
        pltpu.make_async_copy(near.at[1], k1.at[:, :, pl.ds(HALOS[1], SPAN)], sems.at[3]),
    ]
    for c in copies:
        c.start()
    for c in copies:
        c.wait()
    core, t = lax.axis_index("sp") % 2, lax.axis_index("tp")
    for i in range(SPAN // BLOCK):
        rows = slice(i * BLOCK, (i + 1) * BLOCK)
        biases = [bias_of(g, i) for g in range(2)]
        for some in (PLACES[:3], PLACES[3:]):
            items = []
            for g, held in enumerate((k0, k1)):
                keys = slice(i * BLOCK, (i + 1) * BLOCK + HALOS[g])
                items += [
                    (q[g, b, rows, cols], held[0, b, keys, cols], held[1, b, keys, cols], biases[g]) for b, _, cols in some
                ]
            found = attend(items)
            for n, (b, h, cols) in enumerate(some):
                o, l = joined(*found[n], *found[n + 3])
                o, l = joined(o, l, other[b, rows, cols], logs[b, rows, cols])
                mixed[b, rows, cols] = o.astype(jnp.bfloat16)
                weights[i, 2 * b + h : 2 * b + h + 1, :] = jnp.transpose(l)[0:1]
    kept[...] = weights[core]
    sent[...] = weights[1 - core]
    for d, out in enumerate((c0, c1, c2, c3)):
        for far in range(2):
            whose = core if far == 0 else 1 - core
            at = pl.multiple_of(whose * HALF + ((t + d) % RING) * PIECE, PIECE)
            out[far] = mixed[:, pl.ds(at, PIECE), :]


def attend_near(q, near, tail, other, logs):
    piece = bf(2, BATCHES, PIECE, COLS)
    line = jax.ShapeDtypeStruct((2 * BATCHES, BLOCK), jnp.float32)
    return pl.pallas_call(
        near_body, out_shape=(piece,) * 4 + (line,) * 2, grid=(1,),
        in_specs=[pl.BlockSpec((2, BATCHES, SPAN, COLS), lambda i: (0, 0, 0, 0)), ANY, ANY, VMEM, VMEM],
        out_specs=(VMEM,) * 6,
        scratch_shapes=[
            pltpu.VMEM((2, BATCHES, HALOS[0] + SPAN, COLS), jnp.bfloat16),
            pltpu.VMEM((2, BATCHES, HALOS[1] + SPAN, COLS), jnp.bfloat16),
            pltpu.VMEM((BATCHES, SPAN, COLS), jnp.bfloat16),
            pltpu.VMEM((2, 2 * BATCHES, BLOCK), jnp.float32),
            pltpu.SemaphoreType.DMA((4,)),
        ],
        compiler_params=PARAMS, name="attend_near",
    )(q, near, tail, other, logs)


def pick_body(a0, a1, a2, a3, out, sems):
    copies = [
        pltpu.make_async_copy(a.at[:, GROUPS], out.at[pl.ds(RING * e, RING)], sems.at[e])
        for e, a in enumerate((a0, a1, a2, a3))
    ]
    for c in copies:
        c.start()
    for c in copies:
        c.wait()


def pick(lines):
    return pl.pallas_call(
        pick_body, out_shape=bf(16, ROWS, COLS), in_specs=[ANY] * 4, out_specs=VMEM,
        scratch_shapes=[pltpu.SemaphoreType.DMA((4,))], compiler_params=PARAMS, name="pick",
    )(*lines)


def final_body(*refs):
    received, lines, ours, crossed = refs[:4], refs[4:12], refs[12:15], refs[15:18]
    keep, send, w_all, sems = refs[18:]
    core = lax.axis_index("sp") % 2
    part = WIDTH // RING
    half = BATCHES * PIECE
    count = part // ROWS
    copies = []
    for n in range(2 * RING):
        whose = core if n < RING else 1 - core
        others = ours if n < RING else crossed
        for j in range(RING):
            k = place_of(whose, j, n % RING, 0)
            at = n * RING + j
            copies.append(pltpu.make_async_copy(lines[n].at[j, GROUPS], w_all.at[0, k], sems.at[0, at]))
            for d, piece in enumerate(others, 1):
                source = piece.at[(n % RING) * RING + j]
                copies.append(pltpu.make_async_copy(source, w_all.at[d, k], sems.at[d, at]))
    for c in copies:
        c.start()
    for c in copies:
        c.wait()
    rows = [r[...].reshape(2 * half, COLS) for r in received]
    for n in range(RING):
        cols = slice(n * part, (n + 1) * part)
        acc = None
        for d in range(RING):
            block = w_all[d, n * count : (n + 1) * count].reshape(part, COLS)
            y = lax.dot_general(rows[d], block, (((1,), (1,)), ((), ())), preferred_element_type=jnp.float32)
            acc = y if acc is None else acc + y
        acc = acc.astype(jnp.bfloat16)
        keep[:, :, cols] = acc[:half].reshape(BATCHES, PIECE, part)
        send[:, :, cols] = acc[half:].reshape(BATCHES, PIECE, part)


def finish(received, lines, pieces, crossed):
    shape = bf(BATCHES, PIECE, WIDTH)
    return pl.pallas_call(
        final_body, out_shape=(shape, shape), in_specs=[VMEM] * 4 + [ANY] * 14, out_specs=(VMEM,) * 2,
        scratch_shapes=[
            pltpu.VMEM((RING, WIDTH // ROWS, ROWS, COLS), jnp.bfloat16), pltpu.SemaphoreType.DMA((RING, 32)),
        ],
        compiler_params=PARAMS, name="finish",
    )(*received, *lines, *pieces, *crossed)


def joined_cores(mine, theirs):
    core = lax.axis_index("sp") % 2
    return jnp.where(core == 0, jnp.concatenate((mine, theirs), 0), jnp.concatenate((theirs, mine), 0))


def merge_body(mine, theirs, out):
    core = lax.axis_index("sp") % 2
    out[pl.ds(core * BATCHES, BATCHES)] = mine[...]
    out[pl.ds((1 - core) * BATCHES, BATCHES)] = theirs[...]


def merged(mine, theirs):
    return pl.pallas_call(
        merge_body, out_shape=bf(2 * BATCHES, PIECE, WIDTH), in_specs=[VMEM] * 2, out_specs=VMEM,
        compiler_params=PARAMS, name="merge",
    )(mine, theirs)


def ring_of(a):
    came = {d: turned(a, d) for d in (1, 3, 2)}
    return [a, came[1], came[2], came[3]]


def spread(own, kind):
    near = {d: lax.ppermute(own, "sp", first_leg(d, kind)) for d in (1, 3, 2)}
    line = jnp.stack((own, near[1], near[2], near[3]))
    far = {d: lax.ppermute(line, "sp", second_leg(d, kind)) for d in (1, 3, 2)}
    lines = [line, far[1], far[2], far[3]]
    return lines + [swapped(a) for a in lines]


def spread_halves(own):
    near = {d: lax.ppermute(own, "sp", first_leg(d, 0)) for d in (1, 3, 2)}
    halves = []
    for part, way in ((slice(0, NEAR), 1), (slice(NEAR, None), 3)):
        line = jnp.stack([a[part] for a in (own, near[1], near[2], near[3])])
        far = {d: lax.ppermute(line, "sp", second_leg(d, 0)) for d in (1, 3)}
        far[2] = lax.ppermute(far[way], "sp", second_leg(way, 0))
        lines = [line, far[1], far[2], far[3]]
        halves.append(lines + [swapped(a) for a in lines])
    return halves


def layer(tokens, norm_gain, w_query, w_key, w_value, w_out):
    wide_own, rest_own = pack(w_query, w_key, w_value, w_out)

    core = lax.axis_index("sp") % 2
    tokens = jnp.transpose(tokens, (1, 0, 2))
    send = lax.dynamic_slice_in_dim(tokens, (1 - core) * BATCHES, BATCHES, 0)
    other = swapped(send)
    wide_lines = spread(wide_own, 0)
    late, early = norm_rows(tokens, other, norm_gain)
    late, early = ring_of(late), ring_of(early)
    pair_lines, query_lines = spread_halves(rest_own)

    wide_late = project_wide(late, wide_lines)
    far_late = from_behind(wide_late, 2)
    back_late = from_behind(wide_late, 1)
    wide_early = project_wide(early, wide_lines)
    back_early = from_behind(wide_early, 1)
    near, near_tail = project_near(early, late, pair_lines)
    near_tail = from_behind(near_tail, 1)
    outs = ring_of(pick(query_lines[:RING]))[1:]
    queries = project_queries(early, late, query_lines)
    wide_out, wide_logs = attend_wide(queries, wide_early, wide_late, back_early, back_late, far_late)
    *combined, kept, sent = attend_near(queries, near, near_tail, wide_out, wide_logs)

    received = [combined[0]] + [turned(combined[d], d) for d in (1, 2, 3)]
    mixed_mine, mixed_sent = finish(received, query_lines, outs, [swapped(a) for a in outs])
    mixed = merged(mixed_mine, swapped(mixed_sent))

    log_weight = joined_cores(kept, swapped(sent)).reshape(2 * BATCHES, 2, BLOCK)
    return (jnp.transpose(mixed, (1, 0, 2)), jnp.transpose(log_weight, (2, 0, 1)))


def solution(mesh):
    in_specs = (
        P(("sp", "tp"), None, None),
        P(),
        P(None, "sp", "tp"),
        P(None, "sp", "tp"),
        P(None, "sp", "tp"),
        P("tp", "sp"),
    )
    out_specs = (P(("sp", "tp"), None, None), P("sp", None, "tp"))
    return jax.shard_map(layer, mesh=mesh, in_specs=in_specs, out_specs=out_specs, check_vma=False)
```
